128 devices in a mesh: sp: 16 (over z, y), dp: 8 (over x, core).
Axes of the slice: x: 4, y: 4, z: 4, core: 2. Of those that a mesh axis runs over, the one named last changes fastest.
Arguments:
- query_first: bfloat16 [8, 2048, 1024], P('dp', 'sp'), may hold values from -200 to 200
- key_first: bfloat16 [8, 2048, 1024], P('dp', 'sp'), may hold values from -8 to 8
- query_second: bfloat16 [8, 2048, 1024], P('dp', 'sp'), may hold values from -200 to 200
- key_second: bfloat16 [8, 2048, 1024], P('dp', 'sp'), may hold values from -8 to 8
- value_rows: bfloat16 [8, 2048, 2048], P('dp', 'sp'), may hold values from -6 to 6
- mix_lambda: float32 [16], replicated, may hold values from 0.3 to 0.8
- head_gain: float32 [128], replicated, may hold values from 0.1 to 1.9
- residual: bfloat16 [8, 2048, 2048], P('dp', 'sp'), may hold values from -6 to 6
- out_weight: bfloat16 [2048, 2048], replicated, may hold values from -0.125 to 0.125
- norm_gain: float32 [2048], replicated, may hold values from 0.1 to 1.9
- routes: int32 [8, 2048, 4], P('dp', 'sp'), may hold values from 0 to 127, all different within a row; in each aligned block of 128 rows (0 to 127, 128 to 255, ..., all dimensions but the last counted through in order) at most 6 rows name the same one
- route_weights: float32 [8, 2048, 4], P('dp', 'sp'), may hold values from 0.1 to 1
- gate_weight: bfloat16 [128, 2048, 1024], P(('sp', 'dp')), may hold values from -0.375 to 0.375
- up_weight: bfloat16 [128, 2048, 1024], P(('sp', 'dp')), may hold values from -0.375 to 0.375
- down_weight: bfloat16 [128, 1024, 2048], P(('sp', 'dp')), may hold values from -0.046875 to 0.046875
Outputs:
- layer_out: bfloat16 [8, 2048, 2048], P('dp', 'sp')
The draws below stay inside these ranges and needn't reach their ends.
Inputs may be any that keep to these rules, and one draw needn't show every extreme that they name: `routes`: within the rows of one device (aligned blocks of 128 positions of a sequence) no expert is named more than 6 times, a bound that some block reaches.
All inputs are finite; a program needn't handle non-finite values.
Results may differ from the reference program's by a relative error of at most 0.0075.
Values may be sent and summed in bfloat16 or wider, within the bound.
A program may use at most 128 MiB of HBM per device.

```python
import math
import jax
import jax.numpy as jnp
import numpy as np
from jax import lax

D = 2048
H = 16
HD = 64
HV = 128
FF = 1024
TOPK = 4
TOK_DEV = 128
LENGTH = 2048
SEQS = 8
EXPERTS = 128
CAP = 6
N_SP = 16
N_DP = 8


def drawn(key, which):
    shape = (SEQS, LENGTH, H * HD)
    keys = jnp.clip(jax.random.normal(jax.random.fold_in(key, 10 + which), shape, jnp.float32) * 1.3, -8.0, 8.0)
    queries = jnp.clip(jax.random.normal(jax.random.fold_in(key, 20 + which), shape, jnp.float32) * 1.3, -8.0, 8.0)
    return (queries, keys)


def draw_query_first(key, part):
    return drawn(key, 0)[0].astype(jnp.bfloat16)


def draw_key_first(key, part):
    return drawn(key, 0)[1].astype(jnp.bfloat16)


def draw_query_second(key, part):
    return drawn(key, 1)[0].astype(jnp.bfloat16)


def draw_key_second(key, part):
    return drawn(key, 1)[1].astype(jnp.bfloat16)


def block_scale(key, dims, cuts, least, top_value):
    factor_of = 1.0
    for dim, blocks in cuts:
        draws = jax.random.uniform(jax.random.fold_in(jax.random.fold_in(key, 6), dim), (blocks,), jnp.float32, least / len(cuts), top_value / len(cuts))
        factor_of = factor_of * jnp.repeat(jnp.exp(draws), dims[dim] // blocks).reshape((-1,) + (1,) * (len(dims) - 1 - dim))
    return factor_of


def shared_out(own_key, own, number, rows, amount, top, bound, slope):
    ranking = jax.random.permutation(own_key, amount)
    heavy_load, ordinary = load_shares(amount, rows * top, bound, slope, True), load_shares(amount, rows * top, bound, slope, False)
    places = jnp.arange(amount)

    def named(lengths, offset_by):
        used = int((lengths > 0).sum())
        fixed = max(1, used // 4)
        passed = fixed + (places - fixed + offset_by * (used - fixed)) % max(1, amount - fixed)
        return jnp.zeros((amount,), jnp.int32).at[ranking[jnp.where(places < fixed, places, passed)]].set(jnp.asarray(lengths, jnp.int32))

    lengths = jnp.where(number % 4 == 0, named(heavy_load, number // 4), named(ordinary, number - number // 4 - 1))
    mixed = jax.random.permutation(jax.random.fold_in(own, 3), amount)
    giver, sink = mixed[0:amount // 2 * 2:2], mixed[1:amount // 2 * 2:2]
    slack = jnp.minimum(lengths[giver] - 1, bound - lengths[sink]) // 2
    slack = jnp.where((giver == ranking[0]) | (sink == ranking[0]) | (lengths[sink] == 0), 0, jnp.maximum(slack, 0))
    passed = jax.random.randint(jax.random.fold_in(own, 4), (amount // 2,), 0, 1 << 20) % (slack + 1)
    lengths = lengths.at[giver].add(-passed).at[sink].add(passed)
    labels = jnp.searchsorted(jnp.cumsum(lengths), jnp.arange(rows * top), side="right").astype(jnp.int32)
    listing = labels.reshape(top, rows).T
    listing = listing[jax.random.permutation(jax.random.fold_in(own, 1), rows)]
    offset_by = jax.random.randint(jax.random.fold_in(own, 2), (rows, 1), 0, top)
    return jnp.take_along_axis(listing, (jnp.arange(top)[None, :] + offset_by) % top, axis=1)


def load_shares(amount, total, most, skew, full):
    weights = [(1 << 20) // math.isqrt(grade ** skew) + 1 for grade in range(1, amount + 1)]
    largest = most if full else min(most, max(-(-total // amount), total * weights[0] // sum(weights)))
    least = 1 if total - largest >= amount - 1 else 0
    holding, surplus = [largest] + [least] * (amount - 1), total - largest - least * (amount - 1)
    while surplus > 0:
        candidates = [i for i in range(1, amount) if holding[i] < largest] or [i for i in range(1, amount) if holding[i] < most]
        pool, remaining = sum([weights[i] for i in candidates]), surplus
        for i in candidates:
            addition = min(most - holding[i], max(1, remaining * weights[i] // pool), surplus)
            holding[i] = holding[i] + addition
            surplus = surplus - addition
    return np.array(holding)


def bell_draw(rng, extent, deviation, bound, split=(), kind=jnp.bfloat16):
    values = jax.random.normal(rng, extent, jnp.float32) * deviation
    if len(split) > 0:
        values = block_scale(rng, extent, split, -0.22, 0.18) * values
    return jnp.clip(values, min=-bound, max=bound).astype(kind)


def setup_inputs(seed: int = 0) -> dict:
    key_list = jax.random.split(jax.random.key(seed), 16)
    query_first = draw_query_first(jax.random.fold_in(key_list[15], 71), 0)
    key_first = draw_key_first(jax.random.fold_in(key_list[15], 71), 0)
    query_second = draw_query_second(jax.random.fold_in(key_list[15], 71), 0)
    key_second = draw_key_second(jax.random.fold_in(key_list[15], 71), 0)
    value_rows = bell_draw(key_list[4], (SEQS, LENGTH, H * HV), 1.0, 6.0, ((0, 8), (1, 16)))
    mix_lambda = jnp.clip(jax.random.uniform(key_list[5], (H,), jnp.float32, 0.3, 0.8), 0.3, 0.8)
    head_gain = jnp.clip(1.0 + 0.18 * jax.random.normal(key_list[6], (HV,), jnp.float32), 0.1, 1.9)
    residual = bell_draw(key_list[7], (SEQS, LENGTH, D), 1.0, 6.0, ((0, 8), (1, 16)))
    out_weight = bell_draw(key_list[8], (H * HV, D), (H * HV) ** -0.5, 0.125)
    norm_gain = jnp.clip(1.0 + 0.18 * jax.random.normal(key_list[9], (D,), jnp.float32), 0.1, 1.9)
    routes_keys = jax.random.split(jax.random.fold_in(key_list[10], 1), SEQS * LENGTH // TOK_DEV)
    routes_turns = jax.random.permutation(jax.random.fold_in(key_list[10], 3), SEQS * LENGTH // TOK_DEV)
    routes = jax.vmap(lambda own, number: shared_out(jax.random.fold_in(key_list[10], 2), own, number, TOK_DEV, EXPERTS, TOPK, CAP, 2))(routes_keys, routes_turns).reshape((SEQS, LENGTH, TOPK))
    route_weights = jnp.clip(0.1 + 0.9 * jax.random.uniform(key_list[11], (SEQS, LENGTH, TOPK), jnp.float32) ** block_scale(key_list[11], (SEQS, LENGTH, TOPK), ((0, 8), (1, 16)), -0.2, 0.2), 0.1, 1.0)
    gate_weight = bell_draw(key_list[12], (EXPERTS, D, FF), (D // 9) ** -0.5, 0.375, ((0, 128),))
    up_weight = bell_draw(key_list[13], (EXPERTS, D, FF), (D // 9) ** -0.5, 0.375, ((0, 128),))
    down_weight = bell_draw(key_list[14], (EXPERTS, FF, D), (16 * FF) ** -0.5, 0.046875, ((0, 128),))
    return dict(query_first=query_first, key_first=key_first, query_second=query_second, key_second=key_second, value_rows=value_rows, mix_lambda=mix_lambda, head_gain=head_gain, residual=residual, out_weight=out_weight, norm_gain=norm_gain, routes=routes, route_weights=route_weights, gate_weight=gate_weight, up_weight=up_weight, down_weight=down_weight)


def head_attention(operands):
    query_one, key_one, query_two, key_two, value_head, weight_two, head_gain = operands
    length = query_one.shape[0]
    qblock = min(length, max(512, length // 16))
    scale = HD ** (-0.5)
    keypos = jnp.arange(length, dtype=jnp.int32)

    def block(start):
        rows = start * qblock + jnp.arange(qblock, dtype=jnp.int32)
        q_one = lax.dynamic_slice_in_dim(query_one, (start * qblock).astype(jnp.int32), qblock, 0)
        q_two = lax.dynamic_slice_in_dim(query_two, (start * qblock).astype(jnp.int32), qblock, 0)
        score_one = jnp.dot(q_one, key_one.T, preferred_element_type=jnp.float32) * scale
        score_two = jnp.dot(q_two, key_two.T, preferred_element_type=jnp.float32) * scale
        visible = keypos[None, :] <= rows[:, None]
        prob_one = jax.nn.softmax(jnp.where(visible, score_one, -1e+30), axis=-1)
        prob_two = jax.nn.softmax(jnp.where(visible, score_two, -1e+30), axis=-1)
        mixture = (prob_one - weight_two * prob_two).astype(jnp.bfloat16)
        head_raw = jnp.dot(mixture, value_head, preferred_element_type=jnp.float32)
        factor = lax.rsqrt(lax.optimization_barrier(jnp.mean(head_raw * head_raw, axis=-1, keepdims=True)) + 1e-06)
        return (head_raw * factor * head_gain).astype(jnp.bfloat16)
    return lax.map(block, jnp.arange(length // qblock, dtype=jnp.int32)).reshape(length, HV)

def reference(query_first, key_first, query_second, key_second, value_rows, mix_lambda, head_gain, residual, out_weight, norm_gain, routes, route_weights, gate_weight, up_weight, down_weight):

    def by_head(array, width):
        return array.reshape(SEQS, LENGTH, H, width).transpose(0, 2, 1, 3).reshape(SEQS * H, LENGTH, width)
    gains = jnp.broadcast_to(head_gain, (SEQS * H, HV))
    heads = lax.map(head_attention, (by_head(query_first, HD), by_head(key_first, HD), by_head(query_second, HD), by_head(key_second, HD), by_head(value_rows, HV), jnp.tile(mix_lambda, SEQS), gains))
    head_out = heads.reshape(SEQS, H, LENGTH, HV).transpose(0, 2, 1, 3).reshape(SEQS * LENGTH, H * HV)
    attn = jnp.dot(head_out, out_weight, preferred_element_type=jnp.float32)
    mixed = residual.reshape(SEQS * LENGTH, D).astype(jnp.float32) + attn
    normed = (mixed * lax.rsqrt(lax.optimization_barrier(jnp.mean(mixed * mixed, axis=-1, keepdims=True)) + 1e-06) * norm_gain).astype(jnp.bfloat16)
    expert_ids = routes.reshape(-1)
    weights = route_weights.reshape(-1)
    total = expert_ids.shape[0]
    order = jnp.argsort(expert_ids, stable=True).astype(jnp.int32)
    counts = jnp.bincount(expert_ids, length=EXPERTS).astype(jnp.int32)
    starts = (jnp.cumsum(counts) - counts).astype(jnp.int32)
    room = CAP * N_SP * N_DP
    offsets = jnp.arange(room, dtype=jnp.int32)

    def expert_step(acc, operands):
        expert, w_gate, w_up, w_down = operands
        slots = jnp.minimum(starts[expert] + offsets, total - 1)
        valid = offsets < counts[expert]
        picks = order[slots]
        tokens = picks // TOPK
        rows = normed[tokens]
        gate = jnp.dot(rows, w_gate, preferred_element_type=jnp.float32)
        upper = jnp.dot(rows, w_up, preferred_element_type=jnp.float32)
        clamped = jnp.minimum(gate, 7.0)
        hidden = ((jnp.clip(upper, -7.0, 7.0) + 1.0) * clamped * jax.nn.sigmoid(1.702 * clamped)).astype(jnp.bfloat16)
        expert_out = jnp.dot(hidden, w_down, preferred_element_type=jnp.float32).astype(jnp.bfloat16)
        scaled = jnp.where(valid, weights[picks], 0.0)[:, None] * expert_out.astype(jnp.float32)
        return (acc.at[tokens].add(scaled), None)
    routed, _ = lax.scan(expert_step, jnp.zeros((SEQS * LENGTH, D), jnp.float32), (jnp.arange(EXPERTS, dtype=jnp.int32), gate_weight, up_weight, down_weight))
    return (mixed + routed).astype(jnp.bfloat16).reshape(SEQS, LENGTH, D)
```

```python
import functools
import jax
import jax.numpy as jnp
from jax import lax
from jax.experimental import pallas as pl
from jax.experimental.pallas import tpu as pltpu
from jax.sharding import PartitionSpec as P

MESH = pl.DeviceIdType.MESH
RING = 4
CAP = 6
OFFSETS = (
    (0, 1), (1, 0), (0, 3), (3, 0), (1, 1), (3, 3), (1, 3), (3, 1),
    (0, 2), (2, 0), (1, 2), (2, 1), (3, 2), (2, 3), (2, 2),
)
CHUNKS = 4


def moe_kernel(
    head_ref, res_ref, wo_hbm, gain_ref, meta_ref, wg_hbm, wu_hbm, wd_hbm,
    out_ref,
    wg, wu, wd, nrm, mixed, gath, slab, xin, gacc, uacc, hid, back, rin,
    part_out, part_in, sum_out, sum_in, own, pick, wsel, meta,
    wsem, meta_s, meta_r, xs, xr, cs, cr, ds, dr, bs, br, ps, pr, ts, tr,
):
    f32, bf16 = jnp.float32, jnp.bfloat16
    sp, dp = lax.axis_index("sp"), lax.axis_index("dp")
    z, y = sp // RING, sp % RING
    x, c = dp // 2, dp % 2
    partner = x * 2 + (1 - c)
    rows, width = res_ref.shape
    n = CHUNKS
    cw = width // n
    slots = slab.shape[1]
    nsp = slab.shape[0]
    ndp = gath.shape[0]
    half = wg.shape[1]

    def cols(k):
        return pl.ds(pl.multiple_of(k * cw, cw), cw)

    def peer(i, sign=1):
        dz, dy = OFFSETS[i]
        return ((z + sign * dz + RING) % RING) * RING + (y + sign * dy + RING) % RING

    def xpeer(i, sign=1):
        return (x + sign * (i + 1) + RING) % RING

    def remote(src, dst, ssem, rsem, to):
        return pltpu.make_async_remote_copy(
            src_ref=src, dst_ref=dst, send_sem=ssem, recv_sem=rsem,
            device_id=to, device_id_type=MESH,
        )

    barrier = pltpu.get_barrier_semaphore()
    for i in range(nsp - 1):
        pl.semaphore_signal(barrier, inc=1, device_id=(peer(i), dp), device_id_type=MESH)
    for i in range(1, ndp):
        pl.semaphore_signal(barrier, inc=1, device_id=(sp, (dp + i) % ndp), device_id_type=MESH)

    wo_a = pltpu.make_async_copy(wo_hbm.at[:, pl.ds(0, half)], wg, wsem.at[0])
    wo_b = pltpu.make_async_copy(wo_hbm.at[:, pl.ds(half, half)], wu, wsem.at[1])
    wd_c = pltpu.make_async_copy(wd_hbm, wd, wsem.at[2])
    wg_c = pltpu.make_async_copy(wg_hbm, wg, wsem.at[3])
    wu_c = pltpu.make_async_copy(wu_hbm, wu, wsem.at[4])
    wo_a.start()
    wo_b.start()
    wd_c.start()

    pl.semaphore_wait(barrier, nsp - 1 + ndp - 1)

    def meta_copy(i, src):
        return remote(meta_ref, meta.at[src], meta_s.at[i], meta_r.at[i], (sp, (dp + i) % ndp))

    for i in range(1, ndp):
        meta_copy(i, dp).start()
    meta[dp] = meta_ref[...]

    tile = 256
    square = jnp.zeros((rows, 128), f32)

    def project(weights, base, t, total):
        at = pl.ds(pl.multiple_of(t * tile, tile), tile)
        to = pl.ds(pl.multiple_of(base + t * tile, tile), tile)
        value = jnp.dot(head_ref[...], weights[:, at], preferred_element_type=f32)
        value = value + res_ref[:, to].astype(f32)
        mixed[:, to] = value
        sq = value * value
        return total + sq[:, :128] + sq[:, 128:]

    wo_a.wait()
    square = lax.fori_loop(0, half // tile, lambda t, v: project(wg, 0, t, v), square)
    wg_c.start()
    wo_b.wait()
    square = lax.fori_loop(0, half // tile, lambda t, v: project(wu, half, t, v), square)
    wu_c.start()
    factor = lax.rsqrt(jnp.sum(square, axis=1, keepdims=True) / width + 1e-06)

    def gx(k, i, src):
        return remote(
            nrm.at[:, cols(k)], gath.at[src * 2 + c, :, cols(k)], xs.at[k, i], xr.at[k, i],
            (sp, xpeer(i) * 2 + c),
        )

    def gown(k):
        return remote(
            nrm.at[:, cols(k)], gath.at[dp, :, cols(k)], cs.at[k, 3], cr.at[k, 3], (sp, partner)
        )

    def gfwd(k, i, core):
        at = (xpeer(i, -1) * 2 + core)
        return remote(
            gath.at[at, :, cols(k)], gath.at[at, :, cols(k)], cs.at[k, i], cr.at[k, i],
            (sp, partner),
        )

    def gsend(k):
        for i in (0, 2, 1):
            gx(k, i, x).start()
        gown(k).start()

    for k in range(n):
        nrm[:, cols(k)] = (mixed[:, cols(k)] * factor * gain_ref[:, cols(k)]).astype(bf16)
        if k > 0:
            gsend(k - 1)
    gath[dp] = nrm[...]
    gsend(n - 1)

    for i in range(1, ndp):
        meta_copy(i, (dp - i + ndp) % ndp).wait_recv()
    before = (
        lax.broadcasted_iota(jnp.int32, (rows, rows), 0)
        < lax.broadcasted_iota(jnp.int32, (rows, rows), 1)
    ).astype(bf16)
    expert = (lax.broadcasted_iota(jnp.int32, (nsp, rows), 0) * ndp + dp).astype(f32)
    place = lax.broadcasted_iota(jnp.int32, (nsp, slots, rows), 1).astype(f32)

    def table(b, carry):
        info = meta[b]
        named = jnp.zeros((nsp, rows), f32)
        weight = jnp.zeros((nsp, rows), f32)
        for t in range(RING):
            hit = (info[t : t + 1, :] == expert).astype(f32)
            named = named + hit
            weight = weight + hit * info[t + RING : t + RING + 1, :]
        rank = jnp.dot(named.astype(bf16), before, preferred_element_type=f32)
        slot = jnp.where(named > 0.0, rank + (b * CAP).astype(f32), -1.0)
        match = (slot[:, None, :] == place).astype(f32)
        at = pl.ds(pl.multiple_of(b * rows, rows), rows)
        pick[:, at] = match.reshape(nsp * slots, rows).astype(bf16)
        scaled = (match * weight[:, None, :]).reshape(nsp * slots, rows)
        wsel[(b % 2) * RING + b // 2] = jnp.transpose(scaled).astype(bf16)
        return carry

    lax.fori_loop(0, ndp, table, 0)
    gacc[...] = jnp.zeros_like(gacc)
    uacc[...] = jnp.zeros_like(uacc)

    def forward(k):
        for i in (0, 2, 1):
            gx(k, i, xpeer(i, -1)).wait_recv()
            gfwd(k, i, c).start()

    def exchange(out_buf, in_buf, ssem, rsem, k, i, src, dst):
        return remote(
            out_buf.at[dst, :, cols(k)], in_buf.at[src, :, cols(k)], ssem.at[k, i], rsem.at[k, i],
            (dst, dp),
        )

    def send_all(out_buf, in_buf, ssem, rsem, k):
        for i in range(nsp - 1):
            exchange(out_buf, in_buf, ssem, rsem, k, i, sp, peer(i)).start()

    def wait_all(out_buf, in_buf, ssem, rsem, k):
        for i in range(nsp - 1):
            exchange(out_buf, in_buf, ssem, rsem, k, i, peer(i, -1), peer(i)).wait_recv()

    def build(k):
        for i in range(3):
            gfwd(k, i, 1 - c).wait_recv()
        remote(
            nrm.at[:, cols(k)], gath.at[partner, :, cols(k)], cs.at[k, 3], cr.at[k, 3], (sp, partner)
        ).wait_recv()
        tokens = gath[:, :, cols(k)].reshape(ndp * rows, cw)
        group = nsp // 4

        def one(g, carry):
            sel = pick[pl.ds(pl.multiple_of(g * group * slots, group * slots), group * slots), :]
            made = jnp.dot(sel, tokens, preferred_element_type=f32).astype(bf16)
            slab[pl.ds(g * group, group), :, cols(k)] = made.reshape(group, slots, cw)
            return carry

        lax.fori_loop(0, 4, one, 0)
        xin[sp, :, cols(k)] = slab[sp, :, cols(k)]

    def expert_in(k):
        wait_all(slab, xin, ds, dr, k)

        def one(t, carry):
            at = pl.ds(pl.multiple_of(t * tile, tile), tile)
            taken = xin[:, :, cols(k)].reshape(nsp * slots, cw)
            gacc[:, at] += jnp.dot(taken, wg[cols(k), at], preferred_element_type=f32)
            uacc[:, at] += jnp.dot(taken, wu[cols(k), at], preferred_element_type=f32)
            return carry

        lax.fori_loop(0, half // tile, one, 0)

    forward(0)

    def dispatch(k, carry):
        build(k)
        send_all(slab, xin, ds, dr, k)

        @pl.when(k + 1 < n)
        def _():
            forward(k + 1)

        @pl.when(k == 1)
        def _():
            wg_c.wait()
            wu_c.wait()

        @pl.when(k > 0)
        def _():
            expert_in(k - 1)

        return carry

    lax.fori_loop(0, n, dispatch, 0)
    expert_in(n - 1)

    def unit(t, carry):
        at = pl.ds(pl.multiple_of(t * 32, 32), 32)
        gate = jnp.minimum(gacc[at, :], 7.0)
        upper = jnp.clip(uacc[at, :], -7.0, 7.0) + 1.0
        hid[at, :] = (upper * gate / (1.0 + jnp.exp(-1.702 * gate))).astype(bf16)
        return carry

    lax.fori_loop(0, nsp * slots // 32, unit, 0)
    wd_c.wait()

    def down(k, carry):
        def one(t, inner):
            at = pl.ds(pl.multiple_of(k * cw + t * tile, tile), tile)
            made = jnp.dot(hid[...], wd[:, at], preferred_element_type=f32).astype(bf16)
            back[:, :, at] = made.reshape(nsp, slots, tile)
            return inner

        lax.fori_loop(0, cw // tile, one, 0)
        rin[sp, :, cols(k)] = back[sp, :, cols(k)]
        send_all(back, rin, bs, br, k)
        return carry

    lax.fori_loop(0, n, down, 0)

    def part(k):
        return remote(
            part_out.at[:, :, cols(k)], part_in.at[:, :, cols(k)], ps.at[k], pr.at[k], (sp, partner)
        )

    def total(k, i, src):
        return remote(
            sum_out.at[xpeer(i), :, cols(k)], sum_in.at[src, :, cols(k)], ts.at[k, i], tr.at[k, i],
            (sp, xpeer(i) * 2 + c),
        )

    def weighted(core, k):
        sel = wsel[pl.ds(core * RING, RING)].reshape(RING * rows, nsp * slots)
        taken = rin[:, :, cols(k)].reshape(nsp * slots, cw)
        return jnp.dot(sel, taken, preferred_element_type=f32).reshape(RING, rows, cw)

    def finish(k):
        value = mixed[:, cols(k)]
        for i in range(3):
            total(k, i, xpeer(i, -1)).wait_recv()
            value = value + sum_in[xpeer(i, -1), :, cols(k)].astype(f32)
        out_ref[:, cols(k)] = value.astype(bf16)

    def combine(k, carry):
        wait_all(back, rin, bs, br, k)
        part_out[:, :, cols(k)] = weighted(1 - c, k).astype(bf16)
        own[...] = weighted(c, k)
        part(k).start()
        part(k).wait_recv()
        mixed[:, cols(k)] += own[x] + part_in[x, :, cols(k)].astype(f32)
        sum_out[:, :, cols(k)] = (own[...] + part_in[:, :, cols(k)].astype(f32)).astype(bf16)
        for i in (1, 0, 2):
            total(k, i, x).start()

        @pl.when(k > 0)
        def _():
            finish(k - 1)

        return carry

    lax.fori_loop(0, n, combine, 0)
    finish(n - 1)

    for i in range(1, ndp):
        meta_copy(i, dp).wait_send()

    def drain(k, carry):
        for i in range(3):
            gx(k, i, x).wait_send()
            gfwd(k, i, c).wait_send()
            total(k, i, x).wait_send()
        gown(k).wait_send()
        part(k).wait_send()
        for i in range(nsp - 1):
            exchange(slab, xin, ds, dr, k, i, sp, peer(i)).wait_send()
            exchange(back, rin, bs, br, k, i, sp, peer(i)).wait_send()
        return carry

    lax.fori_loop(0, n, drain, 0)


def after_attention(heads_out, residual, out_weight, norm_gain, meta, gate_weight, up_weight, down_weight, nsp, ndp):
    rows, width = residual.shape
    hidden = gate_weight.shape[1]
    slots = CAP * ndp
    n = CHUNKS
    bf16, f32 = jnp.bfloat16, jnp.float32
    vmem = pl.BlockSpec(memory_space=pltpu.VMEM)
    hbm = pl.BlockSpec(memory_space=pl.ANY)
    dma = pltpu.SemaphoreType.DMA
    return pl.pallas_call(
        moe_kernel,
        out_shape=jax.ShapeDtypeStruct((rows, width), bf16),
        in_specs=[vmem, vmem, hbm, vmem, vmem, hbm, hbm, hbm],
        out_specs=vmem,
        scratch_shapes=[
            pltpu.VMEM((width, hidden), bf16),
            pltpu.VMEM((width, hidden), bf16),
            pltpu.VMEM((hidden, width), bf16),
            pltpu.VMEM((rows, width), bf16),
            pltpu.VMEM((rows, width), f32),
            pltpu.VMEM((ndp, rows, width), bf16),
            pltpu.VMEM((nsp, slots, width), bf16),
            pltpu.VMEM((nsp, slots, width), bf16),
            pltpu.VMEM((nsp * slots, hidden), f32),
            pltpu.VMEM((nsp * slots, hidden), f32),
            pltpu.VMEM((nsp * slots, hidden), bf16),
            pltpu.VMEM((nsp, slots, width), bf16),
            pltpu.VMEM((nsp, slots, width), bf16),
            pltpu.VMEM((RING, rows, width), bf16),
            pltpu.VMEM((RING, rows, width), bf16),
            pltpu.VMEM((RING, rows, width), bf16),
            pltpu.VMEM((RING, rows, width), bf16),
            pltpu.VMEM((RING, rows, width // n), f32),
            pltpu.VMEM((nsp * slots, ndp * rows), bf16),
            pltpu.VMEM((ndp, rows, nsp * slots), bf16),
            pltpu.VMEM((ndp, 8, rows), f32),
            dma((5,)), dma((ndp,)), dma((ndp,)),
            dma((n, 3)), dma((n, 3)), dma((n, 4)), dma((n, 4)),
            dma((n, nsp)), dma((n, nsp)), dma((n, nsp)), dma((n, nsp)),
            dma((n,)), dma((n,)), dma((n, 3)), dma((n, 3)),
        ],
        compiler_params=pltpu.CompilerParams(
            collective_id=1, has_side_effects=True, vmem_limit_bytes=64 * 1000 * 1000
        ),
        name="experts",
    )(heads_out, residual, out_weight, norm_gain[None, :], meta, gate_weight, up_weight, down_weight)


def sent_together(arrays, axis, split_dim, concat_dim, along):
    widths = [a.shape[along] for a in arrays]
    both = jnp.concatenate(arrays, axis=along)
    out = lax.all_to_all(both, axis, split_axis=split_dim, concat_axis=concat_dim, tiled=True)
    return tuple(jnp.split(out, [sum(widths[:k]) for k in range(1, len(widths))], axis=along))


def on_device(
    query_first,
    key_first,
    query_second,
    key_second,
    value_rows,
    mix_lambda,
    head_gain,
    residual,
    out_weight,
    norm_gain,
    routes,
    route_weights,
    gate_weight,
    up_weight,
    down_weight,
):
    tok_rows = query_first.shape[1]
    heads = mix_lambda.shape[0]
    query_one, key_one, query_two, key_two, value_head = sent_together(
        (
            query_first[0].reshape(tok_rows, heads, -1),
            key_first[0].reshape(tok_rows, heads, -1),
            query_second[0].reshape(tok_rows, heads, -1),
            key_second[0].reshape(tok_rows, heads, -1),
            value_rows[0].reshape(tok_rows, heads, -1),
        ),
        "sp",
        1,
        0,
        2,
    )
    length = query_one.shape[0]
    local = query_one.shape[1]
    value_width = value_head.shape[2]
    scale = query_one.shape[2] ** (-0.5)
    first_head = lax.axis_index("sp") * local
    weight_two = lax.dynamic_slice_in_dim(mix_lambda, first_head, local)[:, None, None]
    qblock = min(length, max(512, length // 16))
    outputs = []
    for step in range(length // qblock):
        begin = step * qblock
        finish = begin + qblock
        score_one = (
            jnp.einsum(
                "qhd,khd->hqk",
                query_one[begin:finish],
                key_one[:finish],
                preferred_element_type=jnp.float32,
            )
            * scale
        )
        score_two = (
            jnp.einsum(
                "qhd,khd->hqk",
                query_two[begin:finish],
                key_two[:finish],
                preferred_element_type=jnp.float32,
            )
            * scale
        )
        visible = jnp.arange(finish)[None, :] <= (begin + jnp.arange(qblock))[:, None]
        prob_one = jax.nn.softmax(jnp.where(visible[None], score_one, -1e30), axis=-1)
        prob_two = jax.nn.softmax(jnp.where(visible[None], score_two, -1e30), axis=-1)
        mixture = (prob_one - weight_two * prob_two).astype(jnp.bfloat16)
        head_raw = jnp.einsum(
            "hqk,khe->qhe", mixture, value_head[:finish], preferred_element_type=jnp.float32
        )
        factor = lax.rsqrt(jnp.mean(head_raw * head_raw, axis=-1, keepdims=True) + 1e-06)
        outputs.append((head_raw * factor * head_gain).astype(jnp.bfloat16))
    head_out = jnp.concatenate(outputs, axis=0)
    returned = lax.all_to_all(head_out, "sp", split_axis=0, concat_axis=1, tiled=True)
    meta = jnp.concatenate([routes[0].T.astype(jnp.float32), route_weights[0].T], axis=0)
    out = after_attention(
        returned.reshape(tok_rows, heads * value_width),
        residual[0],
        out_weight,
        norm_gain,
        meta,
        gate_weight[0],
        up_weight[0],
        down_weight[0],
        lax.axis_size("sp"),
        lax.axis_size("dp"),
    )
    return out[None]


def solution(mesh):
    return jax.shard_map(
        on_device,
        mesh=mesh,
        in_specs=(
            P("dp", "sp", None),
            P("dp", "sp", None),
            P("dp", "sp", None),
            P("dp", "sp", None),
            P("dp", "sp", None),
            P(),
            P(),
            P("dp", "sp", None),
            P(),
            P(),
            P("dp", "sp", None),
            P("dp", "sp", None),
            P(("sp", "dp"), None, None),
            P(("sp", "dp"), None, None),
            P(("sp", "dp"), None, None),
        ),
        out_specs=P("dp", "sp", None),
        check_vma=False,
    )
```

```python
import functools
import jax
import jax.numpy as jnp
from jax import lax
from jax.experimental import pallas as pl
from jax.experimental.pallas import tpu as pltpu
from jax.sharding import PartitionSpec as P

MESH = pl.DeviceIdType.MESH
RING = 4
CAP = 6
OFFSETS = (
    (0, 1), (1, 0), (0, 3), (3, 0), (1, 1), (3, 3), (1, 3), (3, 1),
    (0, 2), (2, 0), (1, 2), (2, 1), (3, 2), (2, 3), (2, 2),
)
CHUNKS = 4


def layer_kernel(
    q1_hbm, k1_hbm, q2_hbm, k2_hbm, v_hbm, lambda_ref, hgain_ref,
    res_ref, wo_hbm, gain_ref, meta_ref, wg_hbm, wu_hbm, wd_hbm,
    out_ref,
    q1, k1, q2, k2, vals, packed, keys, valt, hsend, head_ref,
    wg, wu, wd, nrm, mixed, gath, slab, xin, acc, hid, back, rin,
    part_out, part_in, sum_out, sum_in, own, pick, wsel, meta,
    lsem, as_, ar, hs, hr,
    wsem, meta_s, meta_r, xs, xr, cs, cr, ds, dr, bs, br, ps, pr, ts, tr,
):
    f32, bf16 = jnp.float32, jnp.bfloat16
    sp, dp = lax.axis_index("sp"), lax.axis_index("dp")
    z, y = sp // RING, sp % RING
    x, c = dp // 2, dp % 2
    partner = x * 2 + (1 - c)
    rows, width = res_ref.shape
    n = CHUNKS
    cw = width // n
    slots = slab.shape[1]
    nsp = slab.shape[0]
    ndp = gath.shape[0]
    half = wg.shape[1]

    def cols(k):
        return pl.ds(pl.multiple_of(k * cw, cw), cw)

    def peer(i, sign=1):
        dz, dy = OFFSETS[i]
        return ((z + sign * dz + RING) % RING) * RING + (y + sign * dy + RING) % RING

    def xpeer(i, sign=1):
        return (x + sign * (i + 1) + RING) % RING

    def remote(src, dst, ssem, rsem, to):
        return pltpu.make_async_remote_copy(
            src_ref=src, dst_ref=dst, send_sem=ssem, recv_sem=rsem,
            device_id=to, device_id_type=MESH,
        )

    barrier = pltpu.get_barrier_semaphore()
    for i in range(nsp - 1):
        pl.semaphore_signal(barrier, inc=1, device_id=(peer(i), dp), device_id_type=MESH)
    for i in range(1, ndp):
        pl.semaphore_signal(barrier, inc=1, device_id=(sp, (dp + i) % ndp), device_id_type=MESH)

    loads = [
        pltpu.make_async_copy(src, dst, lsem.at[i])
        for i, (src, dst) in enumerate(
            ((q1_hbm, q1), (q2_hbm, q2), (k1_hbm, k1), (k2_hbm, k2), (v_hbm, vals))
        )
    ]
    for load in loads:
        load.start()
    wo_a = pltpu.make_async_copy(wo_hbm.at[:, pl.ds(0, half)], wg, wsem.at[0])
    wo_b = pltpu.make_async_copy(wo_hbm.at[:, pl.ds(half, half)], wu, wsem.at[1])
    wd_c = pltpu.make_async_copy(wd_hbm, wd, wsem.at[2])
    wg_c = pltpu.make_async_copy(wg_hbm, wg, wsem.at[3])
    wu_c = pltpu.make_async_copy(wu_hbm, wu, wsem.at[4])
    wo_a.start()
    wo_b.start()
    wd_c.start()

    hd = q1.shape[1] // nsp
    hv = vals.shape[1] // nsp
    for load in loads:
        load.wait()
    for g in range(nsp // 2):
        two = slice(g * 2 * hd, (g + 1) * 2 * hd)
        for base, first, second in ((0, q1, q2), (2 * hd, k1, k2)):
            a, b = first[:, two], second[:, two]
            packed[2 * g, :, base : base + 2 * hd] = jnp.concatenate([a[:, :hd], b[:, :hd]], axis=1)
            packed[2 * g + 1, :, base : base + 2 * hd] = jnp.concatenate(
                [a[:, hd:], b[:, hd:]], axis=1
            )
    for h in range(nsp):
        packed[h, :, 4 * hd :] = vals[:, h * hv : (h + 1) * hv]
    keys[sp] = packed[sp]

    pl.semaphore_wait(barrier, nsp - 1 + ndp - 1)

    def qkv(dst, src):
        return remote(packed.at[dst], keys.at[src], as_.at[dst], ar.at[src], (dst, dp))

    for i in range(nsp - 1):
        qkv(peer(i), sp).start()

    def meta_copy(i, src):
        return remote(meta_ref, meta.at[src], meta_s.at[i], meta_r.at[i], (sp, (dp + i) % ndp))

    for i in range(1, ndp):
        meta_copy(i, dp).start()
    meta[dp] = meta_ref[...]

    block = 2 * rows
    blocks = nsp // 2
    lam = lambda_ref[sp]
    scale = hd ** (-0.5) * 1.4426950408889634

    def heads(dst, src):
        at = pl.ds(pl.multiple_of(src * hv, hv), hv)
        return remote(hsend.at[dst], head_ref.at[:, at], hs.at[dst], hr.at[src], (dst, dp))

    def folded(value, op):
        return op(value.reshape(-1, 8, value.shape[1]), axis=0)

    def attend(i, carry):
        for half_block in range(2):
            src = 2 * i + half_block

            @pl.when(src != sp)
            def _():
                qkv(src, src).wait_recv()

        pair = pl.ds(2 * i, 2)
        turned = jnp.transpose(keys[pair, :, 4 * hd :].reshape(block, hv).astype(f32))
        valt[:, pl.ds(pl.multiple_of(i * block, block), block)] = turned.astype(bf16)
        query = keys[pair, :, : 2 * hd].reshape(block, 2 * hd)
        lane = lax.broadcasted_iota(jnp.int32, (block, 2 * hd), 1)
        zero = jnp.zeros_like(query)
        both = jnp.concatenate(
            [jnp.where(lane < hd, query, zero), jnp.where(lane < hd, zero, query)], axis=0
        )

        def score(j):
            key = keys[pl.ds(2 * j, 2), :, 2 * hd : 4 * hd].reshape(block, 2 * hd)
            return lax.dot_general(
                key, both, (((1,), (1,)), ((), ())), preferred_element_type=f32
            )

        def at(j):
            return pl.ds(pl.multiple_of(j * block, block), block)

        def scores(j, top):
            value = score(j)
            acc[at(j), :] = value
            return jnp.maximum(top, folded(value, jnp.max))

        top = lax.fori_loop(0, i, scores, jnp.full((8, 2 * block), -1e30, f32))
        below = lax.broadcasted_iota(jnp.int32, (block, block), 0)
        seen = below <= lax.broadcasted_iota(jnp.int32, (block, block), 1)
        value = jnp.where(jnp.concatenate([seen, seen], axis=1), score(i), -1e30)
        acc[at(i), :] = value
        top = jnp.maximum(top, folded(value, jnp.max))
        top = jnp.max(top, axis=0, keepdims=True)

        def powers(j, total):
            value = jnp.exp2((acc[at(j), :] - top) * scale)
            acc[at(j), :] = value
            return total + folded(value, jnp.sum)

        total = lax.fori_loop(0, i + 1, powers, jnp.zeros((8, 2 * block), f32))
        total = jnp.sum(total, axis=0, keepdims=True)
        first = 1.0 / total[:, :block]
        second = lam / total[:, block:]

        def values(j, raw):
            mix = (acc[at(j), :block] * first - acc[at(j), block:] * second).astype(bf16)
            return raw + jnp.dot(valt[:, at(j)], mix, preferred_element_type=f32)

        raw = lax.fori_loop(0, i + 1, values, jnp.zeros((hv, block), f32))
        size = lax.rsqrt(jnp.mean(raw * raw, axis=0, keepdims=True) + 1e-06)
        done = (jnp.transpose(raw * size) * hgain_ref[...]).astype(bf16)
        hsend[pair] = done.reshape(2, rows, hv)
        for half_block in range(2):
            dst = 2 * i + half_block

            @pl.when(dst != sp)
            def _():
                heads(dst, sp).start()

            @pl.when(dst == sp)
            def _():
                head_ref[:, pl.ds(pl.multiple_of(sp * hv, hv), hv)] = hsend[dst]

        return carry

    lax.fori_loop(0, blocks, attend, 0)
    for i in range(nsp - 1):
        heads(peer(i, -1), peer(i, -1)).wait_recv()

    tile = 256
    square = jnp.zeros((rows, 128), f32)

    def project(weights, base, t, total):
        at = pl.ds(pl.multiple_of(t * tile, tile), tile)
        to = pl.ds(pl.multiple_of(base + t * tile, tile), tile)
        value = jnp.dot(head_ref[...], weights[:, at], preferred_element_type=f32)
        value = value + res_ref[:, to].astype(f32)
        mixed[:, to] = value
        sq = value * value
        return total + sq[:, :128] + sq[:, 128:]

    wo_a.wait()
    square = lax.fori_loop(0, half // tile, lambda t, v: project(wg, 0, t, v), square)
    wg_c.start()
    wo_b.wait()
    square = lax.fori_loop(0, half // tile, lambda t, v: project(wu, half, t, v), square)
    wu_c.start()
    factor = lax.rsqrt(jnp.sum(square, axis=1, keepdims=True) / width + 1e-06)

    def gx(k, i, src):
        return remote(
            nrm.at[:, cols(k)], gath.at[src * 2 + c, :, cols(k)], xs.at[k, i], xr.at[k, i],
            (sp, xpeer(i) * 2 + c),
        )

    def gown(k):
        return remote(
            nrm.at[:, cols(k)], gath.at[dp, :, cols(k)], cs.at[k, 3], cr.at[k, 3], (sp, partner)
        )

    def gfwd(k, i, core):
        at = (xpeer(i, -1) * 2 + core)
        return remote(
            gath.at[at, :, cols(k)], gath.at[at, :, cols(k)], cs.at[k, i], cr.at[k, i],
            (sp, partner),
        )

    def gsend(k):
        for i in (0, 2, 1):
            gx(k, i, x).start()
        gown(k).start()

    for k in range(n):
        nrm[:, cols(k)] = (mixed[:, cols(k)] * factor * gain_ref[:, cols(k)]).astype(bf16)
        if k > 0:
            gsend(k - 1)
    gath[dp] = nrm[...]
    gsend(n - 1)

    for i in range(1, ndp):
        meta_copy(i, (dp - i + ndp) % ndp).wait_recv()
    before = (
        lax.broadcasted_iota(jnp.int32, (rows, rows), 0)
        < lax.broadcasted_iota(jnp.int32, (rows, rows), 1)
    ).astype(bf16)
    expert = (lax.broadcasted_iota(jnp.int32, (nsp, rows), 0) * ndp + dp).astype(f32)
    place = lax.broadcasted_iota(jnp.int32, (nsp, slots, rows), 1).astype(f32)

    def table(b, carry):
        info = meta[b]
        named = jnp.zeros((nsp, rows), f32)
        weight = jnp.zeros((nsp, rows), f32)
        for t in range(RING):
            hit = (info[t : t + 1, :] == expert).astype(f32)
            named = named + hit
            weight = weight + hit * info[t + RING : t + RING + 1, :]
        rank = jnp.dot(named.astype(bf16), before, preferred_element_type=f32)
        slot = jnp.where(named > 0.0, rank + (b * CAP).astype(f32), -1.0)
        match = (slot[:, None, :] == place).astype(f32)
        at = pl.ds(pl.multiple_of(b * rows, rows), rows)
        pick[:, at] = match.reshape(nsp * slots, rows).astype(bf16)
        scaled = (match * weight[:, None, :]).reshape(nsp * slots, rows)
        wsel[(b % 2) * RING + b // 2] = jnp.transpose(scaled).astype(bf16)
        return carry

    lax.fori_loop(0, ndp, table, 0)
    acc[...] = jnp.zeros_like(acc)
    filled = nsp * slots
    span = acc.shape[1]

    def forward(k):
        for i in (0, 2, 1):
            gx(k, i, xpeer(i, -1)).wait_recv()
            gfwd(k, i, c).start()

    def exchange(out_buf, in_buf, ssem, rsem, k, i, src, dst):
        return remote(
            out_buf.at[dst, :, cols(k)], in_buf.at[src, :, cols(k)], ssem.at[k, i], rsem.at[k, i],
            (dst, dp),
        )

    def send_all(out_buf, in_buf, ssem, rsem, k):
        for i in range(nsp - 1):
            exchange(out_buf, in_buf, ssem, rsem, k, i, sp, peer(i)).start()

    def wait_all(out_buf, in_buf, ssem, rsem, k):
        for i in range(nsp - 1):
            exchange(out_buf, in_buf, ssem, rsem, k, i, peer(i, -1), peer(i)).wait_recv()

    def build(k):
        for i in range(3):
            gfwd(k, i, 1 - c).wait_recv()
        remote(
            nrm.at[:, cols(k)], gath.at[partner, :, cols(k)], cs.at[k, 3], cr.at[k, 3], (sp, partner)
        ).wait_recv()
        tokens = gath[:, :, cols(k)].reshape(ndp * rows, cw)
        group = nsp // 4

        def one(g, carry):
            sel = pick[pl.ds(pl.multiple_of(g * group * slots, group * slots), group * slots), :]
            made = jnp.dot(sel, tokens, preferred_element_type=f32).astype(bf16)
            slab[pl.ds(g * group, group), :, cols(k)] = made.reshape(group, slots, cw)
            return carry

        lax.fori_loop(0, 4, one, 0)
        xin[sp, :, cols(k)] = slab[sp, :, cols(k)]

    def expert_in(k):
        wait_all(slab, xin, ds, dr, k)

        def one(t, carry):
            at = pl.ds(pl.multiple_of(t * tile, tile), tile)
            taken = xin[:, :, cols(k)].reshape(nsp * slots, cw)
            per = span // tile
            to = pl.ds(pl.multiple_of((t % per) * tile, tile), tile)
            low = pl.ds(pl.multiple_of((t // per) * filled, filled), filled)
            high = pl.ds(pl.multiple_of((t // per + half // span) * filled, filled), filled)
            acc[low, to] += jnp.dot(taken, wg[cols(k), at], preferred_element_type=f32)
            acc[high, to] += jnp.dot(taken, wu[cols(k), at], preferred_element_type=f32)
            return carry

        lax.fori_loop(0, half // tile, one, 0)

    forward(0)

    def dispatch(k, carry):
        build(k)
        send_all(slab, xin, ds, dr, k)

        @pl.when(k + 1 < n)
        def _():
            forward(k + 1)

        @pl.when(k == 1)
        def _():
            wg_c.wait()
            wu_c.wait()

        @pl.when(k > 0)
        def _():
            expert_in(k - 1)

        return carry

    lax.fori_loop(0, n, dispatch, 0)
    expert_in(n - 1)

    def unit(t, carry):
        at = pl.ds(pl.multiple_of(t * 32, 32), 32)
        for part_of in range(half // span):
            low = pl.ds(pl.multiple_of(part_of * filled + t * 32, 32), 32)
            high = pl.ds(pl.multiple_of((part_of + half // span) * filled + t * 32, 32), 32)
            gate = jnp.minimum(acc[low, :], 7.0)
            upper = jnp.clip(acc[high, :], -7.0, 7.0) + 1.0
            made = upper * gate / (1.0 + jnp.exp(-1.702 * gate))
            hid[at, part_of * span : (part_of + 1) * span] = made.astype(bf16)
        return carry

    lax.fori_loop(0, nsp * slots // 32, unit, 0)
    wd_c.wait()

    def down(k, carry):
        def one(t, inner):
            at = pl.ds(pl.multiple_of(k * cw + t * tile, tile), tile)
            made = jnp.dot(hid[...], wd[:, at], preferred_element_type=f32).astype(bf16)
            back[:, :, at] = made.reshape(nsp, slots, tile)
            return inner

        lax.fori_loop(0, cw // tile, one, 0)
        rin[sp, :, cols(k)] = back[sp, :, cols(k)]
        send_all(back, rin, bs, br, k)
        return carry

    lax.fori_loop(0, n, down, 0)

    def part(k):
        return remote(
            part_out.at[:, :, cols(k)], part_in.at[:, :, cols(k)], ps.at[k], pr.at[k], (sp, partner)
        )

    def total(k, i, src):
        return remote(
            sum_out.at[xpeer(i), :, cols(k)], sum_in.at[src, :, cols(k)], ts.at[k, i], tr.at[k, i],
            (sp, xpeer(i) * 2 + c),
        )

    def weighted(core, k):
        sel = wsel[pl.ds(core * RING, RING)].reshape(RING * rows, nsp * slots)
        taken = rin[:, :, cols(k)].reshape(nsp * slots, cw)
        return jnp.dot(sel, taken, preferred_element_type=f32).reshape(RING, rows, cw)

    def finish(k):
        value = mixed[:, cols(k)]
        for i in range(3):
            total(k, i, xpeer(i, -1)).wait_recv()
            value = value + sum_in[xpeer(i, -1), :, cols(k)].astype(f32)
        out_ref[:, cols(k)] = value.astype(bf16)

    def combine(k, carry):
        wait_all(back, rin, bs, br, k)
        part_out[:, :, cols(k)] = weighted(1 - c, k).astype(bf16)
        own[...] = weighted(c, k)
        part(k).start()
        part(k).wait_recv()
        mixed[:, cols(k)] += own[x] + part_in[x, :, cols(k)].astype(f32)
        sum_out[:, :, cols(k)] = (own[...] + part_in[:, :, cols(k)].astype(f32)).astype(bf16)
        for i in (1, 0, 2):
            total(k, i, x).start()

        @pl.when(k > 0)
        def _():
            finish(k - 1)

        return carry

    lax.fori_loop(0, n, combine, 0)
    finish(n - 1)

    for i in range(nsp - 1):
        qkv(peer(i), sp).wait_send()
        heads(peer(i), sp).wait_send()
    for i in range(1, ndp):
        meta_copy(i, dp).wait_send()

    def drain(k, carry):
        for i in range(3):
            gx(k, i, x).wait_send()
            gfwd(k, i, c).wait_send()
            total(k, i, x).wait_send()
        gown(k).wait_send()
        part(k).wait_send()
        for i in range(nsp - 1):
            exchange(slab, xin, ds, dr, k, i, sp, peer(i)).wait_send()
            exchange(back, rin, bs, br, k, i, sp, peer(i)).wait_send()
        return carry

    lax.fori_loop(0, n, drain, 0)


def on_device(
    query_first,
    key_first,
    query_second,
    key_second,
    value_rows,
    mix_lambda,
    head_gain,
    residual,
    out_weight,
    norm_gain,
    routes,
    route_weights,
    gate_weight,
    up_weight,
    down_weight,
):
    nsp, ndp = lax.axis_size("sp"), lax.axis_size("dp")
    rows, width = residual.shape[1:]
    hidden = gate_weight.shape[2]
    qk = query_first.shape[2]
    hv = head_gain.shape[0]
    packed = 4 * qk // nsp + hv
    slots = CAP * ndp
    n = CHUNKS
    bf16, f32 = jnp.bfloat16, jnp.float32
    meta = jnp.concatenate([routes[0].T.astype(f32), route_weights[0].T], axis=0)
    vmem = pl.BlockSpec(memory_space=pltpu.VMEM)
    smem = pl.BlockSpec(memory_space=pltpu.SMEM)
    hbm = pl.BlockSpec(memory_space=pl.ANY)
    dma = pltpu.SemaphoreType.DMA
    out = pl.pallas_call(
        layer_kernel,
        out_shape=jax.ShapeDtypeStruct((rows, width), bf16),
        in_specs=[hbm] * 5 + [smem, vmem, vmem, hbm, vmem, vmem, hbm, hbm, hbm],
        out_specs=vmem,
        scratch_shapes=[
            pltpu.VMEM((rows, qk), bf16),
            pltpu.VMEM((rows, qk), bf16),
            pltpu.VMEM((rows, qk), bf16),
            pltpu.VMEM((rows, qk), bf16),
            pltpu.VMEM((rows, nsp * hv), bf16),
            pltpu.VMEM((nsp, rows, packed), bf16),
            pltpu.VMEM((nsp, rows, packed), bf16),
            pltpu.VMEM((hv, nsp * rows), bf16),
            pltpu.VMEM((nsp, rows, hv), bf16),
            pltpu.VMEM((rows, nsp * hv), bf16),
            pltpu.VMEM((width, hidden), bf16),
            pltpu.VMEM((width, hidden), bf16),
            pltpu.VMEM((hidden, width), bf16),
            pltpu.VMEM((rows, width), bf16),
            pltpu.VMEM((rows, width), f32),
            pltpu.VMEM((ndp, rows, width), bf16),
            pltpu.VMEM((nsp, slots, width), bf16),
            pltpu.VMEM((nsp, slots, width), bf16),
            pltpu.VMEM((4 * nsp * slots, hidden // 2), f32),
            pltpu.VMEM((nsp * slots, hidden), bf16),
            pltpu.VMEM((nsp, slots, width), bf16),
            pltpu.VMEM((nsp, slots, width), bf16),
            pltpu.VMEM((RING, rows, width), bf16),
            pltpu.VMEM((RING, rows, width), bf16),
            pltpu.VMEM((RING, rows, width), bf16),
            pltpu.VMEM((RING, rows, width), bf16),
            pltpu.VMEM((RING, rows, width // n), f32),
            pltpu.VMEM((nsp * slots, ndp * rows), bf16),
            pltpu.VMEM((ndp, rows, nsp * slots), bf16),
            pltpu.VMEM((ndp, 8, rows), f32),
            dma((5,)), dma((nsp,)), dma((nsp,)), dma((nsp,)), dma((nsp,)),
            dma((5,)), dma((ndp,)), dma((ndp,)),
            dma((n, 3)), dma((n, 3)), dma((n, 4)), dma((n, 4)),
            dma((n, nsp)), dma((n, nsp)), dma((n, nsp)), dma((n, nsp)),
            dma((n,)), dma((n,)), dma((n, 3)), dma((n, 3)),
        ],
        compiler_params=pltpu.CompilerParams(
            collective_id=1, has_side_effects=True, vmem_limit_bytes=67000000
        ),
        name="layer",
    )(
        query_first[0], key_first[0], query_second[0], key_second[0], value_rows[0],
        mix_lambda, head_gain[None, :], residual[0], out_weight, norm_gain[None, :], meta,
        gate_weight[0], up_weight[0], down_weight[0],
    )
    return out[None]


def solution(mesh):
    return jax.shard_map(
        on_device,
        mesh=mesh,
        in_specs=(
            P("dp", "sp", None),
            P("dp", "sp", None),
            P("dp", "sp", None),
            P("dp", "sp", None),
            P("dp", "sp", None),
            P(),
            P(),
            P("dp", "sp", None),
            P(),
            P(),
            P("dp", "sp", None),
            P("dp", "sp", None),
            P(("sp", "dp"), None, None),
            P(("sp", "dp"), None, None),
            P(("sp", "dp"), None, None),
        ),
        out_specs=P("dp", "sp", None),
        check_vma=False,
    )
```

```python
import functools
import jax
import jax.numpy as jnp
from jax import lax
from jax.experimental import pallas as pl
from jax.experimental.pallas import tpu as pltpu
from jax.sharding import PartitionSpec as P

MESH = pl.DeviceIdType.MESH
RING = 4
CAP = 6
OFFSETS = (
    (0, 1), (1, 0), (0, 3), (3, 0), (1, 1), (3, 3), (1, 3), (3, 1),
    (0, 2), (2, 0), (1, 2), (2, 1), (3, 2), (2, 3), (2, 2),
)
CHUNKS = 8


def layer_kernel(
    q1_hbm, k1_hbm, q2_hbm, k2_hbm, v_hbm, lambda_ref, hgain_ref,
    res_ref, wo_hbm, gain_ref, meta_ref, wg_hbm, wu_hbm, wd_hbm,
    out_ref,
    q1, k1, q2, k2, vals, packed, keys, valt, mix, hsend, head_ref,
    wg, wu, wd, nrm, mixed, gath, slab, xin, acc, hid, back, rin,
    part_out, part_in, sum_out, sum_in, own, pick, wsel, meta,
    lsem, as_, ar, hs, hr,
    wsem, meta_s, meta_r, xs, xr, cs, cr, ds, dr, bs, br, ps, pr, ts, tr,
):
    f32, bf16 = jnp.float32, jnp.bfloat16
    sp, dp = lax.axis_index("sp"), lax.axis_index("dp")
    z, y = sp // RING, sp % RING
    x, c = dp // 2, dp % 2
    partner = x * 2 + (1 - c)
    rows, width = res_ref.shape
    n = CHUNKS
    cw = width // n
    slots = slab.shape[1]
    nsp = slab.shape[0]
    ndp = gath.shape[0]
    half = wg.shape[1]

    def cols(k):
        return pl.ds(pl.multiple_of(k * cw, cw), cw)

    def peer(i, sign=1):
        dz, dy = OFFSETS[i]
        return ((z + sign * dz + RING) % RING) * RING + (y + sign * dy + RING) % RING

    def xpeer(i, sign=1):
        return (x + sign * (i + 1) + RING) % RING

    def remote(src, dst, ssem, rsem, to):
        return pltpu.make_async_remote_copy(
            src_ref=src, dst_ref=dst, send_sem=ssem, recv_sem=rsem,
            device_id=to, device_id_type=MESH,
        )

    barrier = pltpu.get_barrier_semaphore()
    for i in range(nsp - 1):
        pl.semaphore_signal(barrier, inc=1, device_id=(peer(i), dp), device_id_type=MESH)
    for i in range(1, ndp):
        pl.semaphore_signal(barrier, inc=1, device_id=(sp, (dp + i) % ndp), device_id_type=MESH)

    loads = [
        pltpu.make_async_copy(src, dst, lsem.at[i])
        for i, (src, dst) in enumerate(
            ((q1_hbm, q1), (q2_hbm, q2), (k1_hbm, k1), (k2_hbm, k2), (v_hbm, vals))
        )
    ]
    for load in loads:
        load.start()
    wo_a = pltpu.make_async_copy(wo_hbm.at[:, pl.ds(0, half)], wg, wsem.at[0])
    wo_b = pltpu.make_async_copy(wo_hbm.at[:, pl.ds(half, half)], wu, wsem.at[1])
    wd_c = pltpu.make_async_copy(wd_hbm, wd, wsem.at[2])
    wg_c = pltpu.make_async_copy(wg_hbm, wg, wsem.at[3])
    wu_c = pltpu.make_async_copy(wu_hbm, wu, wsem.at[4])

    hd = q1.shape[1] // nsp
    hv = vals.shape[1] // nsp
    for load in loads:
        load.wait()
    wo_a.start()
    wo_b.start()
    wd_c.start()
    for g in range(nsp // 2):
        two = slice(g * 2 * hd, (g + 1) * 2 * hd)
        for base, first, second in ((0, q1, q2), (2 * hd, k1, k2)):
            a, b = first[:, two], second[:, two]
            packed[2 * g, :, base : base + 2 * hd] = jnp.concatenate([a[:, :hd], b[:, :hd]], axis=1)
            packed[2 * g + 1, :, base : base + 2 * hd] = jnp.concatenate(
                [a[:, hd:], b[:, hd:]], axis=1
            )
    for h in range(nsp):
        packed[h, :, 4 * hd :] = vals[:, h * hv : (h + 1) * hv]
    keys[sp] = packed[sp]

    pl.semaphore_wait(barrier, nsp - 1 + ndp - 1)

    def qkv(dst, src, which):
        at = pl.ds(0, 4 * hd) if which == 0 else pl.ds(4 * hd, hv)
        return remote(
            packed.at[dst, :, at], keys.at[src, :, at], as_.at[which, dst], ar.at[which, src],
            (dst, dp),
        )

    for which in range(2):
        for i in range(nsp - 1):
            qkv(peer(i), sp, which).start()

    def meta_copy(i, src):
        return remote(meta_ref, meta.at[src], meta_s.at[i], meta_r.at[i], (sp, (dp + i) % ndp))

    for i in range(1, ndp):
        meta_copy(i, dp).start()
    meta[dp] = meta_ref[...]

    block = 2 * rows
    blocks = nsp // 2
    lam = lambda_ref[sp]
    scale = hd ** (-0.5) * 1.4426950408889634

    def heads(dst, src):
        at = pl.ds(pl.multiple_of(src * hv, hv), hv)
        return remote(hsend.at[dst], head_ref.at[:, at], hs.at[dst], hr.at[src], (dst, dp))

    def folded(value, op):
        return op(value.reshape(-1, 8, value.shape[1]), axis=0)

    def at(j):
        return pl.ds(pl.multiple_of(j * block, block), block)

    def arrived(i, which):
        for src in (2 * i, 2 * i + 1):

            @pl.when(src != sp)
            def _():
                qkv(src, src, which).wait_recv()

    below = lax.broadcasted_iota(jnp.int32, (block, 2 * block), 0)
    across = lax.broadcasted_iota(jnp.int32, (block, 2 * block), 1)
    seen = below <= jnp.where(across < block, across, across - block)
    lane = lax.broadcasted_iota(jnp.int32, (block, 2 * hd), 1)

    def attend(i):
        arrived(i, 0)
        query = keys[2 * i : 2 * i + 2, :, : 2 * hd].reshape(block, 2 * hd)
        zero = jnp.zeros_like(query)
        both = jnp.concatenate(
            [jnp.where(lane < hd, query, zero), jnp.where(lane < hd, zero, query)], axis=0
        )
        top = jnp.full((8, 2 * block), -1e30, f32)
        for j in range(i + 1):
            key = keys[2 * j : 2 * j + 2, :, 2 * hd : 4 * hd].reshape(block, 2 * hd)
            value = lax.dot_general(
                key, both, (((1,), (1,)), ((), ())), preferred_element_type=f32
            )
            if j == i:
                value = jnp.where(seen, value, -1e30)
            acc[j * block : (j + 1) * block, :] = value
            top = jnp.maximum(top, folded(value, jnp.max))
        top = jnp.max(top, axis=0, keepdims=True)

        def powers(j, total):
            value = jnp.exp2((acc[at(j), :] - top) * scale)
            acc[at(j), :] = value
            return total + folded(value, jnp.sum)

        total = lax.fori_loop(0, i + 1, powers, jnp.zeros((8, 2 * block), f32))
        total = jnp.sum(total, axis=0, keepdims=True)
        first = 1.0 / total[:, :block]
        second = lam / total[:, block:]

        def mixed_up(j, carry):
            value = acc[at(j), :block] * first - acc[at(j), block:] * second
            mix[i * (i + 1) // 2 + j] = value.astype(bf16)
            return carry

        lax.fori_loop(0, i + 1, mixed_up, 0)

    def gather_values(i):
        arrived(i, 1)
        turned = jnp.transpose(keys[2 * i : 2 * i + 2, :, 4 * hd :].reshape(block, hv).astype(f32))
        valt[:, i * block : (i + 1) * block] = turned.astype(bf16)
        begin = i * (i + 1) // 2
        taken = mix[begin : begin + i + 1].reshape((i + 1) * block, block)
        raw = jnp.dot(valt[:, : (i + 1) * block], taken, preferred_element_type=f32)
        size = lax.rsqrt(jnp.mean(raw * raw, axis=0, keepdims=True) + 1e-06)
        done = (jnp.transpose(raw * size) * hgain_ref[...]).astype(bf16)
        hsend[2 * i : 2 * i + 2] = done.reshape(2, rows, hv)
        for dst in (2 * i, 2 * i + 1):

            @pl.when(dst != sp)
            def _():
                heads(dst, sp).start()

            @pl.when(dst == sp)
            def _():
                head_ref[:, pl.ds(pl.multiple_of(sp * hv, hv), hv)] = hsend[dst]

    for i in range(blocks):
        attend(i)
    for i in range(blocks):
        gather_values(i)
    for i in range(nsp - 1):
        heads(peer(i, -1), peer(i, -1)).wait_recv()

    tile = 256
    square = jnp.zeros((rows, 128), f32)

    def project(weights, base, t, total):
        at = pl.ds(pl.multiple_of(t * tile, tile), tile)
        to = pl.ds(pl.multiple_of(base + t * tile, tile), tile)
        value = jnp.dot(head_ref[...], weights[:, at], preferred_element_type=f32)
        value = value + res_ref[:, to].astype(f32)
        mixed[:, to] = value
        sq = value * value
        return total + sq[:, :128] + sq[:, 128:]

    wo_a.wait()
    square = lax.fori_loop(0, half // tile, lambda t, v: project(wg, 0, t, v), square)
    wg_c.start()
    wo_b.wait()
    square = lax.fori_loop(0, half // tile, lambda t, v: project(wu, half, t, v), square)
    wu_c.start()
    factor = lax.rsqrt(jnp.sum(square, axis=1, keepdims=True) / width + 1e-06)

    def gx(k, i, src):
        return remote(
            nrm.at[:, cols(k)], gath.at[src * 2 + c, :, cols(k)], xs.at[k, i], xr.at[k, i],
            (sp, xpeer(i) * 2 + c),
        )

    def gown(k):
        return remote(
            nrm.at[:, cols(k)], gath.at[dp, :, cols(k)], cs.at[k, 3], cr.at[k, 3], (sp, partner)
        )

    def gfwd(k, i, core):
        at = (xpeer(i, -1) * 2 + core)
        return remote(
            gath.at[at, :, cols(k)], gath.at[at, :, cols(k)], cs.at[k, i], cr.at[k, i],
            (sp, partner),
        )

    def gsend(k):
        for i in (0, 2, 1):
            gx(k, i, x).start()
        gown(k).start()

    for k in range(n):
        nrm[:, cols(k)] = (mixed[:, cols(k)] * factor * gain_ref[:, cols(k)]).astype(bf16)
        if k > 0:
            gsend(k - 1)
    gath[dp] = nrm[...]
    gsend(n - 1)

    for i in range(1, ndp):
        meta_copy(i, (dp - i + ndp) % ndp).wait_recv()
    before = (
        lax.broadcasted_iota(jnp.int32, (rows, rows), 0)
        < lax.broadcasted_iota(jnp.int32, (rows, rows), 1)
    ).astype(bf16)
    expert = (lax.broadcasted_iota(jnp.int32, (nsp, rows), 0) * ndp + dp).astype(f32)
    place = lax.broadcasted_iota(jnp.int32, (nsp, slots, rows), 1).astype(f32)

    def table(b, carry):
        info = meta[b]
        named = jnp.zeros((nsp, rows), f32)
        weight = jnp.zeros((nsp, rows), f32)
        for t in range(RING):
            hit = (info[t : t + 1, :] == expert).astype(f32)
            named = named + hit
            weight = weight + hit * info[t + RING : t + RING + 1, :]
        rank = jnp.dot(named.astype(bf16), before, preferred_element_type=f32)
        slot = jnp.where(named > 0.0, rank + (b * CAP).astype(f32), -1.0)
        match = (slot[:, None, :] == place).astype(f32)
        at = pl.ds(pl.multiple_of(b * rows, rows), rows)
        pick[:, at] = match.reshape(nsp * slots, rows).astype(bf16)
        scaled = (match * weight[:, None, :]).reshape(nsp * slots, rows)
        wsel[(b % 2) * RING + b // 2] = jnp.transpose(scaled).astype(bf16)
        return carry

    lax.fori_loop(0, ndp, table, 0)
    acc[...] = jnp.zeros_like(acc)
    filled = nsp * slots
    span = acc.shape[1]

    def forward(k):
        for i in (0, 2, 1):
            gx(k, i, xpeer(i, -1)).wait_recv()
            gfwd(k, i, c).start()

    def exchange(out_buf, in_buf, ssem, rsem, k, i, src, dst):
        return remote(
            out_buf.at[dst, :, cols(k)], in_buf.at[src, :, cols(k)], ssem.at[k, i], rsem.at[k, i],
            (dst, dp),
        )

    def send_all(out_buf, in_buf, ssem, rsem, k):
        for i in range(nsp - 1):
            exchange(out_buf, in_buf, ssem, rsem, k, i, sp, peer(i)).start()

    def wait_all(out_buf, in_buf, ssem, rsem, k):
        for i in range(nsp - 1):
            exchange(out_buf, in_buf, ssem, rsem, k, i, peer(i, -1), peer(i)).wait_recv()

    def build(k):
        for i in range(3):
            gfwd(k, i, 1 - c).wait_recv()
        remote(
            nrm.at[:, cols(k)], gath.at[partner, :, cols(k)], cs.at[k, 3], cr.at[k, 3], (sp, partner)
        ).wait_recv()
        tokens = gath[:, :, cols(k)].reshape(ndp * rows, cw)
        group = nsp // 4

        def one(g, carry):
            sel = pick[pl.ds(pl.multiple_of(g * group * slots, group * slots), group * slots), :]
            made = jnp.dot(sel, tokens, preferred_element_type=f32).astype(bf16)
            slab[pl.ds(g * group, group), :, cols(k)] = made.reshape(group, slots, cw)
            return carry

        lax.fori_loop(0, 4, one, 0)
        xin[sp, :, cols(k)] = slab[sp, :, cols(k)]

    def expert_in(k):
        wait_all(slab, xin, ds, dr, k)

        def one(t, carry):
            at = pl.ds(pl.multiple_of(t * tile, tile), tile)
            taken = xin[:, :, cols(k)].reshape(nsp * slots, cw)
            per = span // tile
            to = pl.ds(pl.multiple_of((t % per) * tile, tile), tile)
            low = pl.ds(pl.multiple_of((t // per) * filled, filled), filled)
            high = pl.ds(pl.multiple_of((t // per + half // span) * filled, filled), filled)
            acc[low, to] += jnp.dot(taken, wg[cols(k), at], preferred_element_type=f32)
            acc[high, to] += jnp.dot(taken, wu[cols(k), at], preferred_element_type=f32)
            return carry

        lax.fori_loop(0, half // tile, one, 0)

    def dispatch(k, carry):
        forward(k)
        build(k)
        send_all(slab, xin, ds, dr, k)
        return carry

    lax.fori_loop(0, n, dispatch, 0)
    wg_c.wait()
    wu_c.wait()

    def receive(k, carry):
        expert_in(k)
        return carry

    lax.fori_loop(0, n, receive, 0)

    def unit(t, carry):
        at = pl.ds(pl.multiple_of(t * 32, 32), 32)
        for part_of in range(half // span):
            low = pl.ds(pl.multiple_of(part_of * filled + t * 32, 32), 32)
            high = pl.ds(pl.multiple_of((part_of + half // span) * filled + t * 32, 32), 32)
            gate = jnp.minimum(acc[low, :], 7.0)
            upper = jnp.clip(acc[high, :], -7.0, 7.0) + 1.0
            made = upper * gate / (1.0 + jnp.exp(-1.702 * gate))
            hid[at, part_of * span : (part_of + 1) * span] = made.astype(bf16)
        return carry

    lax.fori_loop(0, nsp * slots // 32, unit, 0)
    wd_c.wait()

    def down(k, carry):
        def one(t, inner):
            at = pl.ds(pl.multiple_of(k * cw + t * tile, tile), tile)
            made = jnp.dot(hid[...], wd[:, at], preferred_element_type=f32).astype(bf16)
            back[:, :, at] = made.reshape(nsp, slots, tile)
            return inner

        lax.fori_loop(0, cw // tile, one, 0)
        rin[sp, :, cols(k)] = back[sp, :, cols(k)]
        send_all(back, rin, bs, br, k)
        return carry

    lax.fori_loop(0, n, down, 0)

    def part(k):
        return remote(
            part_out.at[:, :, cols(k)], part_in.at[:, :, cols(k)], ps.at[k], pr.at[k], (sp, partner)
        )

    def total(k, i, src):
        return remote(
            sum_out.at[xpeer(i), :, cols(k)], sum_in.at[src, :, cols(k)], ts.at[k, i], tr.at[k, i],
            (sp, xpeer(i) * 2 + c),
        )

    def weighted(core, k):
        sel = wsel[pl.ds(core * RING, RING)].reshape(RING * rows, nsp * slots)
        taken = rin[:, :, cols(k)].reshape(nsp * slots, cw)
        return jnp.dot(sel, taken, preferred_element_type=f32).reshape(RING, rows, cw)

    def finish(k):
        value = mixed[:, cols(k)]
        for i in range(3):
            total(k, i, xpeer(i, -1)).wait_recv()
            value = value + sum_in[xpeer(i, -1), :, cols(k)].astype(f32)
        out_ref[:, cols(k)] = value.astype(bf16)

    def combine(k, carry):
        wait_all(back, rin, bs, br, k)
        part_out[:, :, cols(k)] = weighted(1 - c, k).astype(bf16)
        own[...] = weighted(c, k)
        part(k).start()
        part(k).wait_recv()
        mixed[:, cols(k)] += own[x] + part_in[x, :, cols(k)].astype(f32)
        sum_out[:, :, cols(k)] = (own[...] + part_in[:, :, cols(k)].astype(f32)).astype(bf16)
        for i in (1, 0, 2):
            total(k, i, x).start()

        @pl.when(k > 0)
        def _():
            finish(k - 1)

        return carry

    lax.fori_loop(0, n, combine, 0)
    finish(n - 1)

    for i in range(nsp - 1):
        qkv(peer(i), sp, 0).wait_send()
        qkv(peer(i), sp, 1).wait_send()
        heads(peer(i), sp).wait_send()
    for i in range(1, ndp):
        meta_copy(i, dp).wait_send()

    def drain(k, carry):
        for i in range(3):
            gx(k, i, x).wait_send()
            gfwd(k, i, c).wait_send()
            total(k, i, x).wait_send()
        gown(k).wait_send()
        part(k).wait_send()
        for i in range(nsp - 1):
            exchange(slab, xin, ds, dr, k, i, sp, peer(i)).wait_send()
            exchange(back, rin, bs, br, k, i, sp, peer(i)).wait_send()
        return carry

    lax.fori_loop(0, n, drain, 0)


def on_device(
    query_first,
    key_first,
    query_second,
    key_second,
    value_rows,
    mix_lambda,
    head_gain,
    residual,
    out_weight,
    norm_gain,
    routes,
    route_weights,
    gate_weight,
    up_weight,
    down_weight,
):
    nsp, ndp = lax.axis_size("sp"), lax.axis_size("dp")
    rows, width = residual.shape[1:]
    hidden = gate_weight.shape[2]
    qk = query_first.shape[2]
    hv = head_gain.shape[0]
    packed = 4 * qk // nsp + hv
    slots = CAP * ndp
    n = CHUNKS
    bf16, f32 = jnp.bfloat16, jnp.float32
    meta = jnp.concatenate([routes[0].T.astype(f32), route_weights[0].T], axis=0)
    vmem = pl.BlockSpec(memory_space=pltpu.VMEM)
    smem = pl.BlockSpec(memory_space=pltpu.SMEM)
    hbm = pl.BlockSpec(memory_space=pl.ANY)
    dma = pltpu.SemaphoreType.DMA
    out = pl.pallas_call(
        layer_kernel,
        out_shape=jax.ShapeDtypeStruct((rows, width), bf16),
        in_specs=[hbm] * 5 + [smem, vmem, vmem, hbm, vmem, vmem, hbm, hbm, hbm],
        out_specs=vmem,
        scratch_shapes=[
            pltpu.VMEM((rows, qk), bf16),
            pltpu.VMEM((rows, qk), bf16),
            pltpu.VMEM((rows, qk), bf16),
            pltpu.VMEM((rows, qk), bf16),
            pltpu.VMEM((rows, nsp * hv), bf16),
            pltpu.VMEM((nsp, rows, packed), bf16),
            pltpu.VMEM((nsp, rows, packed), bf16),
            pltpu.VMEM((hv, nsp * rows), bf16),
            pltpu.VMEM((nsp * (nsp + 2) // 8, 2 * rows, 2 * rows), bf16),
            pltpu.VMEM((nsp, rows, hv), bf16),
            pltpu.VMEM((rows, nsp * hv), bf16),
            pltpu.VMEM((width, hidden), bf16),
            pltpu.VMEM((width, hidden), bf16),
            pltpu.VMEM((hidden, width), bf16),
            pltpu.VMEM((rows, width), bf16),
            pltpu.VMEM((rows, width), f32),
            pltpu.VMEM((ndp, rows, width), bf16),
            pltpu.VMEM((nsp, slots, width), bf16),
            pltpu.VMEM((nsp, slots, width), bf16),
            pltpu.VMEM((4 * nsp * slots, hidden // 2), f32),
            pltpu.VMEM((nsp * slots, hidden), bf16),
            pltpu.VMEM((nsp, slots, width), bf16),
            pltpu.VMEM((nsp, slots, width), bf16),
            pltpu.VMEM((RING, rows, width), bf16),
            pltpu.VMEM((RING, rows, width), bf16),
            pltpu.VMEM((RING, rows, width), bf16),
            pltpu.VMEM((RING, rows, width), bf16),
            pltpu.VMEM((RING, rows, width // n), f32),
            pltpu.VMEM((nsp * slots, ndp * rows), bf16),
            pltpu.VMEM((ndp, rows, nsp * slots), bf16),
            pltpu.VMEM((ndp, 8, rows), f32),
            dma((5,)), dma((2, nsp)), dma((2, nsp)), dma((nsp,)), dma((nsp,)),
            dma((5,)), dma((ndp,)), dma((ndp,)),
            dma((n, 3)), dma((n, 3)), dma((n, 4)), dma((n, 4)),
            dma((n, nsp)), dma((n, nsp)), dma((n, nsp)), dma((n, nsp)),
            dma((n,)), dma((n,)), dma((n, 3)), dma((n, 3)),
        ],
        compiler_params=pltpu.CompilerParams(
            collective_id=1, has_side_effects=True, vmem_limit_bytes=67000000
        ),
        name="layer",
    )(
        query_first[0], key_first[0], query_second[0], key_second[0], value_rows[0],
        mix_lambda, head_gain[None, :], residual[0], out_weight, norm_gain[None, :], meta,
        gate_weight[0], up_weight[0], down_weight[0],
    )
    return out[None]


def solution(mesh):
    return jax.shard_map(
        on_device,
        mesh=mesh,
        in_specs=(
            P("dp", "sp", None),
            P("dp", "sp", None),
            P("dp", "sp", None),
            P("dp", "sp", None),
            P("dp", "sp", None),
            P(),
            P(),
            P("dp", "sp", None),
            P(),
            P(),
            P("dp", "sp", None),
            P("dp", "sp", None),
            P(("sp", "dp"), None, None),
            P(("sp", "dp"), None, None),
            P(("sp", "dp"), None, None),
        ),
        out_specs=P("dp", "sp", None),
        check_vma=False,
    )
```

```python
import jax
import jax.numpy as jnp
from jax import lax
from jax.experimental import pallas as pl
from jax.experimental.pallas import tpu as pltpu
from jax.sharding import PartitionSpec as P

MESH = pl.DeviceIdType.MESH
RING = 4
CAP = 6
OFFSETS = (
    (0, 1), (1, 0), (0, 3), (3, 0), (1, 1), (3, 3), (1, 3), (3, 1),
    (0, 2), (2, 0), (1, 2), (2, 1), (3, 2), (2, 3), (2, 2),
)
EDGE = 128
WIDE = 256
ENDS = 2


def layer_kernel(
    q1_hbm, k1_hbm, q2_hbm, k2_hbm, v_hbm, lambda_hbm, hgain_hbm,
    res_hbm, wo_hbm, gain_hbm, routes_hbm, rweights_hbm, wg_hbm, wu_hbm, wd_hbm,
    out_hbm,
    q1, k1, q2, k2, vals, lamv, hgain, res, gain, routes, rweights,
    packed, keys, valt, mix, hsend, heads_in,
    wg, wu, wd, mixed, gath, slab, xin, acc, hid, back, rin,
    part_out, part_in, sum_out, sum_in, own, pick, wsel, meta, done_out,
    lsem, as_, ar, hs, hr, osem,
    wsem, meta_s, meta_r, xs, xr, cs, cr, ds, dr, bs, br, ps, pr, ts, tr,
):
    f32, bf16 = jnp.float32, jnp.bfloat16
    sp, dp = lax.axis_index("sp"), lax.axis_index("dp")
    z, y = sp // RING, sp % RING
    x, c = dp // 2, dp % 2
    partner = x * 2 + (1 - c)
    rows, width = res.shape
    nsp, slots = slab.shape[0], slab.shape[1]
    ndp = gath.shape[0]
    filled = nsp * slots
    half = wg.shape[1]
    hd = q1.shape[1] // nsp
    hv = vals.shape[1] // nsp
    wide = (width - 2 * ENDS * EDGE) // WIDE
    n = wide + 2 * ENDS

    def head_chunk(k):
        return (k, pl.multiple_of(k * EDGE, EDGE), EDGE)

    def middle(k):
        return (k, pl.multiple_of(ENDS * EDGE + (k - ENDS) * WIDE, EDGE), WIDE)

    def tail_chunk(k):
        return (k, pl.multiple_of(width - (n - k) * EDGE, EDGE), EDGE)

    def loop(begin, end, step):
        def body(k, carry):
            step(k)
            return carry

        lax.fori_loop(begin, end, body, 0)

    def cols(chunk):
        return pl.ds(chunk[1], chunk[2])

    def peer(i, sign=1):
        dz, dy = OFFSETS[i]
        return ((z + sign * dz + RING) % RING) * RING + (y + sign * dy + RING) % RING

    def xpeer(i, sign=1):
        return (x + sign * (i + 1) + RING) % RING

    def remote(src, dst, ssem, rsem, to):
        return pltpu.make_async_remote_copy(
            src_ref=src, dst_ref=dst, send_sem=ssem, recv_sem=rsem,
            device_id=to, device_id_type=MESH,
        )

    barrier = pltpu.get_barrier_semaphore()
    for i in range(nsp - 1):
        pl.semaphore_signal(barrier, inc=1, device_id=(peer(i), dp), device_id_type=MESH)
    for i in range(1, ndp):
        pl.semaphore_signal(barrier, inc=1, device_id=(sp, (dp + i) % ndp), device_id_type=MESH)

    loads = [
        pltpu.make_async_copy(src, dst, lsem.at[i])
        for i, (src, dst) in enumerate(
            (
                (q1_hbm, q1), (q2_hbm, q2), (k1_hbm, k1), (k2_hbm, k2),
                (routes_hbm, routes), (rweights_hbm, rweights), (v_hbm, vals),
                (lambda_hbm, lamv), (hgain_hbm, hgain), (gain_hbm, gain), (res_hbm, res),
            )
        )
    ]
    for load in loads:
        load.start()
    wo_a = pltpu.make_async_copy(wo_hbm.at[:, pl.ds(0, half)], wg, wsem.at[0])
    wo_b = pltpu.make_async_copy(wo_hbm.at[:, pl.ds(half, half)], wu, wsem.at[1])
    wd_c = pltpu.make_async_copy(wd_hbm, wd, wsem.at[2])
    wg_c = pltpu.make_async_copy(wg_hbm, wg, wsem.at[3])
    wu_c = pltpu.make_async_copy(wu_hbm, wu, wsem.at[4])

    for step, (base, one, two) in enumerate(((0, q1, q2), (2 * hd, k1, k2))):
        loads[2 * step].wait()
        loads[2 * step + 1].wait()
        for g in range(nsp // 2):
            pair = slice(g * 2 * hd, (g + 1) * 2 * hd)
            a, b = one[:, pair], two[:, pair]
            at = slice(base, base + 2 * hd)
            packed[2 * g, :, at] = jnp.concatenate([a[:, :hd], b[:, :hd]], axis=1)
            packed[2 * g + 1, :, at] = jnp.concatenate([a[:, hd:], b[:, hd:]], axis=1)
    loads[4].wait()
    loads[5].wait()
    meta[dp, :RING] = routes[...].astype(f32)
    meta[dp, RING:] = rweights[...]

    pl.semaphore_wait(barrier, nsp - 1 + ndp - 1)

    def qkv(dst, src, which):
        at = pl.ds(0, 4 * hd) if which == 0 else pl.ds(4 * hd, hv)
        return remote(
            packed.at[dst, :, at], keys.at[src, :, at], as_.at[which, dst], ar.at[which, src],
            (dst, dp),
        )

    def meta_copy(i, src):
        return remote(
            meta.at[src], meta.at[src], meta_s.at[i], meta_r.at[i], (sp, (dp + i) % ndp)
        )

    for i in range(nsp - 1):
        qkv(peer(i), sp, 0).start()
    for i in range(1, ndp):
        meta_copy(i, dp).start()
    loads[6].wait()
    for h in range(nsp):
        packed[h, :, 4 * hd :] = vals[:, h * hv : (h + 1) * hv]
    keys[sp] = packed[sp]
    wo_a.start()
    wo_b.start()
    wd_c.start()
    for load in loads[7:]:
        load.wait()

    for i in range(1, ndp):
        meta_copy(i, (dp - i + ndp) % ndp).wait_recv()
    before = (
        lax.broadcasted_iota(jnp.int32, (rows, rows), 0)
        < lax.broadcasted_iota(jnp.int32, (rows, rows), 1)
    ).astype(bf16)
    expert = (lax.broadcasted_iota(jnp.int32, (nsp, rows), 0) * ndp + dp).astype(f32)
    place = lax.broadcasted_iota(jnp.int32, (nsp, slots, rows), 1).astype(f32)

    def table(b, carry):
        info = meta[b]
        named = jnp.zeros((nsp, rows), f32)
        weight = jnp.zeros((nsp, rows), f32)
        for t in range(RING):
            hit = (info[t : t + 1, :] == expert).astype(f32)
            named = named + hit
            weight = weight + hit * info[t + RING : t + RING + 1, :]
        rank = jnp.dot(named.astype(bf16), before, preferred_element_type=f32)
        slot = jnp.where(named > 0.0, rank + (b * CAP).astype(f32), -1.0)
        match = (slot[:, None, :] == place).astype(f32)
        at = pl.ds(pl.multiple_of(b * rows, rows), rows)
        pick[:, at] = match.reshape(filled, rows).astype(bf16)
        scaled = (match * weight[:, None, :]).reshape(filled, rows)
        wsel[(b % 2) * RING + b // 2] = jnp.transpose(scaled).astype(bf16)
        return carry

    lax.fori_loop(0, ndp, table, 0)

    for i in range(nsp - 1):
        qkv(peer(i), sp, 0).wait_send()
    for i in range(nsp - 1):
        qkv(peer(i), sp, 1).start()

    block = 2 * rows
    blocks = nsp // 2
    lane_of = lax.broadcasted_iota(jnp.int32, (1, nsp), 1)
    lam = jnp.sum(jnp.where(lane_of == sp, lamv[...], 0.0), axis=1, keepdims=True)
    scale = hd ** (-0.5) * 1.4426950408889634

    def heads(dst, src):
        at = pl.ds(pl.multiple_of(src * hv, hv), hv)
        return remote(hsend.at[dst], heads_in.at[:, at], hs.at[dst], hr.at[src], (dst, dp))

    def folded(value, op):
        return op(value.reshape(-1, 8, value.shape[1]), axis=0)

    def arrived(i, which):
        for src in (2 * i, 2 * i + 1):

            @pl.when(src != sp)
            def _():
                qkv(src, src, which).wait_recv()

    below = lax.broadcasted_iota(jnp.int32, (block, 2 * block), 0)
    across = lax.broadcasted_iota(jnp.int32, (block, 2 * block), 1)
    seen = below <= jnp.where(across < block, across, across - block)
    lane = lax.broadcasted_iota(jnp.int32, (block, 2 * hd), 1)

    def base(i):
        return 0 if i % 2 == 0 else (blocks - 1) * block

    def tile_of(i, j):
        return slice(base(i) + j * block, base(i) + (j + 1) * block)

    def score(i):
        arrived(i, 0)
        query = keys[2 * i : 2 * i + 2, :, : 2 * hd].reshape(block, 2 * hd)
        zero = jnp.zeros_like(query)
        both = jnp.concatenate(
            [jnp.where(lane < hd, query, zero), jnp.where(lane < hd, zero, query)], axis=0
        )
        top = jnp.full((8, 2 * block), -1e30, f32)
        for j in range(i + 1):
            key = keys[2 * j : 2 * j + 2, :, 2 * hd : 4 * hd].reshape(block, 2 * hd)
            value = lax.dot_general(
                key, both, (((1,), (1,)), ((), ())), preferred_element_type=f32
            )
            if j == i:
                value = jnp.where(seen, value, -1e30)
            acc[tile_of(i, j), :] = value
            top = jnp.maximum(top, folded(value, jnp.max))
        return jnp.max(top, axis=0, keepdims=True)

    def normalize(i, top):
        total = jnp.zeros((8, 2 * block), f32)
        for j in range(i + 1):
            value = jnp.exp2((acc[tile_of(i, j), :] - top) * scale)
            acc[tile_of(i, j), :] = value
            total = total + folded(value, jnp.sum)
        total = jnp.sum(total, axis=0, keepdims=True)
        share = 1.0 / total[:, :block]
        taken = lam / total[:, block:]
        for j in range(i + 1):
            at = tile_of(i, j)
            value = acc[at, :block] * share - acc[at, block:] * taken
            mix[i * (i + 1) // 2 + j] = value.astype(bf16)

    def weigh(i):
        arrived(i, 1)
        turned = jnp.transpose(keys[2 * i : 2 * i + 2, :, 4 * hd :].reshape(block, hv).astype(f32))
        valt[:, i * block : (i + 1) * block] = turned.astype(bf16)
        begin = i * (i + 1) // 2
        tiles = mix[begin : begin + i + 1].reshape((i + 1) * block, block)
        return jnp.dot(valt[:, : (i + 1) * block], tiles, preferred_element_type=f32)

    def settle(i, raw):
        size = lax.rsqrt(jnp.mean(raw * raw, axis=0, keepdims=True) + 1e-06)
        done = (jnp.transpose(raw * size) * hgain[...]).astype(bf16)
        hsend[2 * i : 2 * i + 2] = done.reshape(2, rows, hv)
        for dst in (2 * i, 2 * i + 1):

            @pl.when(dst != sp)
            def _():
                heads(dst, sp).start()

            @pl.when(dst == sp)
            def _():
                heads_in[:, pl.ds(pl.multiple_of(sp * hv, hv), hv)] = hsend[dst]

    def settle_all(which):
        raw = weigh(which[0])
        for n_th, i in enumerate(which):
            following = weigh(which[n_th + 1]) if n_th + 1 < len(which) else None
            settle(i, raw)
            raw = following

    done_to = 0
    top = score(0)
    for i in range(blocks):
        next_top = score(i + 1) if i + 1 < blocks else None
        normalize(i, top)
        top = next_top
        ready = {blocks - 3: i - 1, blocks - 2: i, blocks - 1: i + 1}.get(i, 0)
        if ready > done_to:
            settle_all(range(done_to, ready))
            done_to = ready

    mixed[...] = res[...].astype(f32)
    wo_a.wait()
    wo_b.wait()

    def project(g, carry):
        pair = (g // RING) * RING + (g % RING + 2 * (1 - g // RING)) % RING
        for s in range(2):
            src = 2 * pair + s

            @pl.when(src != sp)
            def _():
                heads(src, src).wait_recv()

        deep = pl.ds(pl.multiple_of(pair * 2 * hv, 2 * hv), 2 * hv)
        part = heads_in[:, deep]
        mixed[:, :half] += jnp.dot(part, wg[deep, :], preferred_element_type=f32)
        mixed[:, half:] += jnp.dot(part, wu[deep, :], preferred_element_type=f32)
        return carry

    lax.fori_loop(0, nsp // 2, project, 0)
    wg_c.start()
    wu_c.start()
    square = jnp.zeros((rows, 128), f32)
    for t in range(width // 128):
        value = mixed[:, t * 128 : (t + 1) * 128]
        square = square + value * value
    factor = lax.rsqrt(jnp.sum(square, axis=1, keepdims=True) / width + 1e-06)

    def gx(chunk, i, src):
        k = chunk[0]
        return remote(
            gath.at[dp, :, cols(chunk)], gath.at[src * 2 + c, :, cols(chunk)], xs.at[k, i], xr.at[k, i],
            (sp, xpeer(i) * 2 + c),
        )

    def gown(chunk, src):
        k = chunk[0]
        return remote(
            gath.at[dp, :, cols(chunk)], gath.at[src, :, cols(chunk)], cs.at[k, 3], cr.at[k, 3],
            (sp, partner),
        )

    def gfwd(chunk, i, core):
        k = chunk[0]
        at = xpeer(i, -1) * 2 + core
        return remote(
            gath.at[at, :, cols(chunk)], gath.at[at, :, cols(chunk)], cs.at[k, i], cr.at[k, i],
            (sp, partner),
        )

    def gsend(chunk):
        for i in (1, 0, 2):
            gx(chunk, i, x).start()
        gown(chunk, dp).start()

    widths = [EDGE] * ENDS + [WIDE] * wide + [EDGE] * ENDS
    static = [(k, sum(widths[:k]), w) for k, w in enumerate(widths)]
    for k, chunk in enumerate(static):
        at = slice(chunk[1], chunk[1] + chunk[2])
        gath[dp, :, at] = (mixed[:, at] * factor * gain[:, at]).astype(bf16)
        if k > 0:
            gsend(static[k - 1])
    gsend(static[-1])
    acc[...] = jnp.zeros_like(acc)

    def exchange(out_buf, in_buf, ssem, rsem, chunk, i, src, dst):
        k = chunk[0]
        return remote(
            out_buf.at[dst, :, cols(chunk)], in_buf.at[src, :, cols(chunk)],
            ssem.at[k, i], rsem.at[k, i], (dst, dp),
        )

    def send_all(out_buf, in_buf, ssem, rsem, chunk):
        for i in range(nsp - 1):
            exchange(out_buf, in_buf, ssem, rsem, chunk, i, sp, peer(i)).start()

    def wait_all(out_buf, in_buf, ssem, rsem, chunk):
        for i in range(nsp - 1):
            exchange(out_buf, in_buf, ssem, rsem, chunk, i, peer(i, -1), peer(i)).wait_recv()

    def dispatch(chunk):
        for i in (0, 2, 1):
            gx(chunk, i, xpeer(i, -1)).wait_recv()
            gfwd(chunk, i, c).start()
        gown(chunk, partner).wait_recv()
        for i in (0, 2, 1):
            gfwd(chunk, i, 1 - c).wait_recv()
        tokens = gath[:, :, cols(chunk)].reshape(ndp * rows, chunk[2])
        group = nsp // 4

        def build(g, carry):
            sel = pick[pl.ds(pl.multiple_of(g * group * slots, group * slots), group * slots), :]
            made = jnp.dot(sel, tokens, preferred_element_type=f32).astype(bf16)
            slab[pl.ds(g * group, group), :, cols(chunk)] = made.reshape(group, slots, chunk[2])
            return carry

        lax.fori_loop(0, 4, build, 0)
        xin[sp, :, cols(chunk)] = slab[sp, :, cols(chunk)]
        send_all(slab, xin, ds, dr, chunk)

    def each(action, end=n):
        loop(0, ENDS, lambda k: action(head_chunk(k)))
        loop(ENDS, ENDS + wide, lambda k: action(middle(k)))
        loop(ENDS + wide, end, lambda k: action(tail_chunk(k)))

    each(dispatch)
    wg_c.wait()
    wu_c.wait()
    tile = 256
    span = acc.shape[1]
    per = span // tile

    def receive(chunk):
        wait_all(slab, xin, ds, dr, chunk)

        def units(t, carry):
            at = pl.ds(pl.multiple_of(t * tile, tile), tile)
            to = pl.ds(pl.multiple_of((t % per) * tile, tile), tile)
            low = pl.ds(pl.multiple_of((t // per) * filled, filled), filled)
            high = pl.ds(pl.multiple_of((t // per + half // span) * filled, filled), filled)
            taken = xin[:, :, cols(chunk)].reshape(filled, chunk[2])
            gate = jnp.dot(taken, wg[cols(chunk), at], preferred_element_type=f32)
            upper = jnp.dot(taken, wu[cols(chunk), at], preferred_element_type=f32)
            acc[low, to] += gate
            acc[high, to] += upper
            return carry

        lax.fori_loop(0, half // tile, units, 0)

    each(receive, n - 1)

    wait_all(slab, xin, ds, dr, static[-1])

    def gated(t, carry):
        at = pl.ds(pl.multiple_of(t * tile, tile), tile)
        to = pl.ds(pl.multiple_of((t % per) * tile, tile), tile)
        low = pl.ds(pl.multiple_of((t // per) * filled, filled), filled)
        high = pl.ds(pl.multiple_of((t // per + half // span) * filled, filled), filled)
        taken = xin[:, :, cols(static[-1])].reshape(filled, EDGE)
        deep = cols(static[-1])
        gate = acc[low, to] + jnp.dot(taken, wg[deep, at], preferred_element_type=f32)
        upper = acc[high, to] + jnp.dot(taken, wu[deep, at], preferred_element_type=f32)
        gate = jnp.minimum(gate, 7.0)
        upper = jnp.clip(upper, -7.0, 7.0) + 1.0
        hid[:, at] = (upper * gate / (1.0 + jnp.exp(-1.702 * gate))).astype(bf16)
        return carry

    lax.fori_loop(0, half // tile, gated, 0)
    wd_c.wait()

    def down(chunk):
        made = jnp.dot(hid[...], wd[:, cols(chunk)], preferred_element_type=f32).astype(bf16)
        back[:, :, cols(chunk)] = made.reshape(nsp, slots, chunk[2])
        rin[sp, :, cols(chunk)] = back[sp, :, cols(chunk)]
        send_all(back, rin, bs, br, chunk)

    each(down)

    def part_copy(chunk):
        k = chunk[0]
        return remote(
            part_out.at[:, :, cols(chunk)], part_in.at[:, :, cols(chunk)], ps.at[k], pr.at[k],
            (sp, partner),
        )

    def total_copy(chunk, i, src):
        k = chunk[0]
        return remote(
            sum_out.at[xpeer(i), :, cols(chunk)], sum_in.at[src, :, cols(chunk)],
            ts.at[k, i], tr.at[k, i], (sp, xpeer(i) * 2 + c),
        )

    def weighted(core, chunk):
        sel = wsel[pl.ds(core * RING, RING)].reshape(RING * rows, filled)
        taken = rin[:, :, cols(chunk)].reshape(filled, chunk[2])
        made = jnp.dot(sel, taken, preferred_element_type=f32)
        return made.reshape(RING, rows, chunk[2])

    def out_copy(chunk):
        return pltpu.make_async_copy(
            done_out.at[:, cols(chunk)], out_hbm.at[:, cols(chunk)], osem.at[chunk[0]]
        )

    def combine(chunk):
        wait_all(back, rin, bs, br, chunk)
        part_out[:, :, cols(chunk)] = weighted(1 - c, chunk).astype(bf16)
        part_copy(chunk).start()
        own[chunk[0] % 2, :, :, : chunk[2]] = weighted(c, chunk)

    def add_parts(chunk):
        part_copy(chunk).wait_recv()
        mine = own.at[chunk[0] % 2]
        for i in (1, 0, 2):
            to = xpeer(i)
            sums = mine[to, :, : chunk[2]] + part_in[to, :, cols(chunk)].astype(f32)
            sum_out[to, :, cols(chunk)] = sums.astype(bf16)
        mixed[:, cols(chunk)] += mine[x, :, : chunk[2]] + part_in[x, :, cols(chunk)].astype(f32)
        for i in (1, 0, 2):
            total_copy(chunk, i, x).start()

    def finish(chunk):
        value = mixed[:, cols(chunk)]
        for i in range(3):
            total_copy(chunk, i, xpeer(i, -1)).wait_recv()
            value = value + sum_in[xpeer(i, -1), :, cols(chunk)].astype(f32)
        done_out[:, cols(chunk)] = value.astype(bf16)
        out_copy(chunk).start()

    def step(chunk, earlier=None):
        combine(chunk)
        if earlier is not None:
            finish(earlier)
        add_parts(chunk)

    begin, end = ENDS, ENDS + wide
    loop(0, begin, lambda k: step(head_chunk(k)))
    loop(begin, 2 * begin, lambda k: step(middle(k), head_chunk(k - ENDS)))
    loop(2 * begin, end, lambda k: step(middle(k), middle(k - ENDS)))
    loop(end, n, lambda k: step(tail_chunk(k)))
    loop(end - ENDS, end, lambda k: finish(middle(k)))
    loop(end, n, lambda k: finish(tail_chunk(k)))

    for i in range(nsp - 1):
        qkv(peer(i), sp, 1).wait_send()
        heads(peer(i), sp).wait_send()
    for i in range(1, ndp):
        meta_copy(i, dp).wait_send()

    def drain(chunk):
        for i in range(3):
            gx(chunk, i, x).wait_send()
            gfwd(chunk, i, c).wait_send()
            total_copy(chunk, i, x).wait_send()
        gown(chunk, dp).wait_send()
        part_copy(chunk).wait_send()
        for i in range(nsp - 1):
            exchange(slab, xin, ds, dr, chunk, i, sp, peer(i)).wait_send()
            exchange(back, rin, bs, br, chunk, i, sp, peer(i)).wait_send()
        out_copy(chunk).wait()

    each(drain)


def on_device(
    query_first,
    key_first,
    query_second,
    key_second,
    value_rows,
    mix_lambda,
    head_gain,
    residual,
    out_weight,
    norm_gain,
    routes,
    route_weights,
    gate_weight,
    up_weight,
    down_weight,
):
    nsp, ndp = lax.axis_size("sp"), lax.axis_size("dp")
    rows, width = residual.shape[1:]
    hidden = gate_weight.shape[2]
    qk = query_first.shape[2]
    hv = head_gain.shape[0]
    packed = 4 * qk // nsp + hv
    slots = CAP * ndp
    filled = slots * nsp
    n = (width - 2 * ENDS * EDGE) // WIDE + 2 * ENDS
    bf16, f32 = jnp.bfloat16, jnp.float32
    hbm = pl.BlockSpec(memory_space=pl.ANY)
    vmem = pltpu.VMEM
    dma = pltpu.SemaphoreType.DMA
    out = pl.pallas_call(
        layer_kernel,
        out_shape=jax.ShapeDtypeStruct((rows, width), bf16),
        in_specs=[hbm] * 15,
        out_specs=hbm,
        scratch_shapes=[
            vmem((rows, qk), bf16), vmem((rows, qk), bf16),
            vmem((rows, qk), bf16), vmem((rows, qk), bf16),
            vmem((rows, nsp * hv), bf16),
            vmem((1, nsp), f32), vmem((1, hv), f32), vmem((rows, width), bf16),
            vmem((1, width), f32), vmem((RING, rows), jnp.int32), vmem((RING, rows), f32),
            vmem((nsp, rows, packed), bf16),
            vmem((nsp, rows, packed), bf16),
            vmem((hv, nsp * rows), bf16),
            vmem((nsp * (nsp + 2) // 8, 2 * rows, 2 * rows), bf16),
            vmem((nsp, rows, hv), bf16),
            vmem((rows, nsp * hv), bf16),
            vmem((width, hidden), bf16), vmem((width, hidden), bf16),
            vmem((hidden, width), bf16),
            vmem((rows, width), f32),
            vmem((ndp, rows, width), bf16),
            vmem((nsp, slots, width), bf16), vmem((nsp, slots, width), bf16),
            vmem((max(4 * filled, (nsp - 1) * 2 * rows), hidden // 2), f32), vmem((filled, hidden), bf16),
            vmem((nsp, slots, width), bf16), vmem((nsp, slots, width), bf16),
            vmem((RING, rows, width), bf16), vmem((RING, rows, width), bf16),
            vmem((RING, rows, width), bf16), vmem((RING, rows, width), bf16),
            vmem((2, RING, rows, WIDE), f32),
            vmem((filled, ndp * rows), bf16),
            vmem((ndp, rows, filled), bf16),
            vmem((ndp, 8, rows), f32),
            vmem((rows, width), bf16),
            dma((11,)), dma((2, nsp)), dma((2, nsp)), dma((nsp,)), dma((nsp,)), dma((n,)),
            dma((5,)), dma((ndp,)), dma((ndp,)),
            dma((n, 3)), dma((n, 3)), dma((n, 4)), dma((n, 4)),
            dma((n, nsp)), dma((n, nsp)), dma((n, nsp)), dma((n, nsp)),
            dma((n,)), dma((n,)), dma((n, 3)), dma((n, 3)),
        ],
        compiler_params=pltpu.CompilerParams(
            collective_id=1, has_side_effects=True, vmem_limit_bytes=67000000
        ),
        name="layer",
    )(
        query_first[0], key_first[0], query_second[0], key_second[0], value_rows[0],
        mix_lambda[None, :], head_gain[None, :], residual[0], out_weight, norm_gain[None, :],
        routes[0].T, route_weights[0].T, gate_weight[0], up_weight[0], down_weight[0],
    )
    return out[None]


def solution(mesh):
    return jax.shard_map(
        on_device,
        mesh=mesh,
        in_specs=(
            P("dp", "sp", None),
            P("dp", "sp", None),
            P("dp", "sp", None),
            P("dp", "sp", None),
            P("dp", "sp", None),
            P(),
            P(),
            P("dp", "sp", None),
            P(),
            P(),
            P("dp", "sp", None),
            P("dp", "sp", None),
            P(("sp", "dp"), None, None),
            P(("sp", "dp"), None, None),
            P(("sp", "dp"), None, None),
        ),
        out_specs=P("dp", "sp", None),
        check_vma=False,
    )
```

```python
import jax
import jax.numpy as jnp
from jax import lax
from jax.experimental import pallas as pl
from jax.experimental.pallas import tpu as pltpu
from jax.sharding import PartitionSpec as P

MESH = pl.DeviceIdType.MESH
RING = 4
CAP = 6
OFFSETS = (
    (0, 1), (1, 0), (0, 3), (3, 0), (1, 1), (3, 3), (1, 3), (3, 1),
    (0, 2), (2, 0), (1, 2), (2, 1), (3, 2), (2, 3), (2, 2),
)
EDGE = 128
WIDE = 256
ENDS = 2


def layer_kernel(
    q1_hbm, k1_hbm, q2_hbm, k2_hbm, v_hbm, lambda_hbm, hgain_hbm,
    res_hbm, wo_hbm, gain_hbm, routes_hbm, rweights_hbm, wg_hbm, wu_hbm, wd_hbm,
    out_hbm,
    q1, k1, q2, k2, vals, lamv, hgain, res, gain, routes, rweights,
    packed, keys, valt, mix, hsend, heads_in,
    wg, wu, wd, mixed, gath, slab, xin, acc, hid, back, rin,
    part_out, part_in, sum_out, sum_in, own, pick, wsel, meta, done_out,
    lsem, as_, ar, hs, hr, osem,
    wsem, meta_s, meta_r, xs, xr, cs, cr, ds, dr, bs, br, ps, pr, ts, tr,
):
    f32, bf16 = jnp.float32, jnp.bfloat16
    sp, dp = lax.axis_index("sp"), lax.axis_index("dp")
    z, y = sp // RING, sp % RING
    x, c = dp // 2, dp % 2
    partner = x * 2 + (1 - c)
    rows, width = res.shape
    nsp, slots = slab.shape[0], slab.shape[1]
    ndp = gath.shape[0]
    filled = nsp * slots
    half = wg.shape[1]
    hd = q1.shape[1] // nsp
    hv = vals.shape[1] // nsp
    wide = (width - 2 * ENDS * EDGE) // WIDE
    n = wide + 2 * ENDS

    def head_chunk(k):
        return (k, pl.multiple_of(k * EDGE, EDGE), EDGE)

    def middle(k):
        return (k, pl.multiple_of(ENDS * EDGE + (k - ENDS) * WIDE, EDGE), WIDE)

    def tail_chunk(k):
        return (k, pl.multiple_of(width - (n - k) * EDGE, EDGE), EDGE)

    def loop(begin, end, step):
        def body(k, carry):
            step(k)
            return carry

        lax.fori_loop(begin, end, body, 0)

    def cols(chunk):
        return pl.ds(chunk[1], chunk[2])

    def peer(i, sign=1):
        dz, dy = OFFSETS[i]
        return ((z + sign * dz + RING) % RING) * RING + (y + sign * dy + RING) % RING

    def xpeer(i, sign=1):
        return (x + sign * (i + 1) + RING) % RING

    def remote(src, dst, ssem, rsem, to):
        return pltpu.make_async_remote_copy(
            src_ref=src, dst_ref=dst, send_sem=ssem, recv_sem=rsem,
            device_id=to, device_id_type=MESH,
        )

    barrier = pltpu.get_barrier_semaphore()
    for i in range(nsp - 1):
        pl.semaphore_signal(barrier, inc=1, device_id=(peer(i), dp), device_id_type=MESH)
    for i in range(1, ndp):
        pl.semaphore_signal(barrier, inc=1, device_id=(sp, (dp + i) % ndp), device_id_type=MESH)

    loads = [
        pltpu.make_async_copy(src, dst, lsem.at[i])
        for i, (src, dst) in enumerate(
            (
                (q1_hbm, q1), (q2_hbm, q2), (k1_hbm, k1), (k2_hbm, k2),
                (routes_hbm, routes), (rweights_hbm, rweights), (v_hbm, vals),
                (lambda_hbm, lamv), (hgain_hbm, hgain), (gain_hbm, gain), (res_hbm, res),
            )
        )
    ]
    for load in loads:
        load.start()
    wo_a = pltpu.make_async_copy(wo_hbm.at[:, pl.ds(0, half)], wg, wsem.at[0])
    wo_b = pltpu.make_async_copy(wo_hbm.at[:, pl.ds(half, half)], wu, wsem.at[1])
    wd_c = pltpu.make_async_copy(wd_hbm, wd, wsem.at[2])
    wg_c = pltpu.make_async_copy(wg_hbm, wg, wsem.at[3])
    wu_c = pltpu.make_async_copy(wu_hbm, wu, wsem.at[4])

    for step, (base, one, two) in enumerate(((0, q1, q2), (2 * hd, k1, k2))):
        loads[2 * step].wait()
        loads[2 * step + 1].wait()
        for g in range(nsp // 2):
            pair = slice(g * 2 * hd, (g + 1) * 2 * hd)
            a, b = one[:, pair], two[:, pair]
            at = slice(base, base + 2 * hd)
            packed[2 * g, :, at] = jnp.concatenate([a[:, :hd], b[:, :hd]], axis=1)
            packed[2 * g + 1, :, at] = jnp.concatenate([a[:, hd:], b[:, hd:]], axis=1)
    loads[4].wait()
    loads[5].wait()
    meta[dp, :RING] = routes[...].astype(f32)
    meta[dp, RING:] = rweights[...]

    pl.semaphore_wait(barrier, nsp - 1 + ndp - 1)

    def qkv(dst, src, which):
        at = pl.ds(0, 4 * hd) if which == 0 else pl.ds(4 * hd, hv)
        return remote(
            packed.at[dst, :, at], keys.at[src, :, at], as_.at[which, dst], ar.at[which, src],
            (dst, dp),
        )

    def meta_copy(i, src):
        return remote(
            meta.at[src], meta.at[src], meta_s.at[i], meta_r.at[i], (sp, (dp + i) % ndp)
        )

    for i in range(nsp - 1):
        qkv(peer(i), sp, 0).start()
    for i in range(1, ndp):
        meta_copy(i, dp).start()
    loads[6].wait()
    for h in range(nsp):
        packed[h, :, 4 * hd :] = vals[:, h * hv : (h + 1) * hv]
    keys[sp] = packed[sp]
    wo_a.start()
    wo_b.start()
    wd_c.start()
    for load in loads[7:]:
        load.wait()

    for i in range(1, ndp):
        meta_copy(i, (dp - i + ndp) % ndp).wait_recv()
    before = (
        lax.broadcasted_iota(jnp.int32, (rows, rows), 0)
        < lax.broadcasted_iota(jnp.int32, (rows, rows), 1)
    ).astype(bf16)
    expert = (lax.broadcasted_iota(jnp.int32, (nsp, rows), 0) * ndp + dp).astype(f32)
    place = lax.broadcasted_iota(jnp.int32, (nsp, slots, rows), 1).astype(f32)

    def table(b, carry):
        info = meta[b]
        named = jnp.zeros((nsp, rows), f32)
        weight = jnp.zeros((nsp, rows), f32)
        for t in range(RING):
            hit = (info[t : t + 1, :] == expert).astype(f32)
            named = named + hit
            weight = weight + hit * info[t + RING : t + RING + 1, :]
        rank = jnp.dot(named.astype(bf16), before, preferred_element_type=f32)
        slot = jnp.where(named > 0.0, rank + (b * CAP).astype(f32), -1.0)
        match = (slot[:, None, :] == place).astype(f32)
        at = pl.ds(pl.multiple_of(b * rows, rows), rows)
        pick[:, at] = match.reshape(filled, rows).astype(bf16)
        scaled = (match * weight[:, None, :]).reshape(filled, rows)
        wsel[(b % 2) * RING + b // 2] = jnp.transpose(scaled).astype(bf16)
        return carry

    lax.fori_loop(0, ndp, table, 0)

    for i in range(nsp - 1):
        qkv(peer(i), sp, 0).wait_send()
    for i in range(nsp - 1):
        qkv(peer(i), sp, 1).start()

    block = 2 * rows
    blocks = nsp // 2
    lane_of = lax.broadcasted_iota(jnp.int32, (1, nsp), 1)
    lam = jnp.sum(jnp.where(lane_of == sp, lamv[...], 0.0), axis=1, keepdims=True)
    scale = hd ** (-0.5) * 1.4426950408889634

    def heads(dst, src):
        at = pl.ds(pl.multiple_of(src * hv, hv), hv)
        return remote(hsend.at[dst], heads_in.at[:, at], hs.at[dst], hr.at[src], (dst, dp))

    def folded(value, op):
        return op(value.reshape(-1, 8, value.shape[1]), axis=0)

    def arrived(i, which):
        for src in (2 * i, 2 * i + 1):

            @pl.when(src != sp)
            def _():
                qkv(src, src, which).wait_recv()

    below = lax.broadcasted_iota(jnp.int32, (block, 2 * block), 0)
    across = lax.broadcasted_iota(jnp.int32, (block, 2 * block), 1)
    seen = below <= jnp.where(across < block, across, across - block)
    lane = lax.broadcasted_iota(jnp.int32, (block, 2 * hd), 1)

    def base(i):
        return 0 if i % 2 == 0 else (blocks - 1) * block

    def tile_of(i, j):
        return slice(base(i) + j * block, base(i) + (j + 1) * block)

    def score(i):
        arrived(i, 0)
        query = keys[2 * i : 2 * i + 2, :, : 2 * hd].reshape(block, 2 * hd)
        zero = jnp.zeros_like(query)
        both = jnp.concatenate(
            [jnp.where(lane < hd, query, zero), jnp.where(lane < hd, zero, query)], axis=0
        )
        top = jnp.full((8, 2 * block), -1e30, f32)
        for j in range(i + 1):
            key = keys[2 * j : 2 * j + 2, :, 2 * hd : 4 * hd].reshape(block, 2 * hd)
            value = lax.dot_general(
                key, both, (((1,), (1,)), ((), ())), preferred_element_type=f32
            )
            if j == i:
                value = jnp.where(seen, value, -1e30)
            acc[tile_of(i, j), :] = value
            top = jnp.maximum(top, folded(value, jnp.max))
        return jnp.max(top, axis=0, keepdims=True)

    def normalize(i, top):
        total = jnp.zeros((8, 2 * block), f32)
        for j in range(i + 1):
            value = jnp.exp2((acc[tile_of(i, j), :] - top) * scale)
            acc[tile_of(i, j), :] = value
            total = total + folded(value, jnp.sum)
        total = jnp.sum(total, axis=0, keepdims=True)
        share = 1.0 / total[:, :block]
        taken = lam / total[:, block:]
        for j in range(i + 1):
            at = tile_of(i, j)
            value = acc[at, :block] * share - acc[at, block:] * taken
            mix[i * (i + 1) // 2 + j] = value.astype(bf16)

    def weigh(i):
        arrived(i, 1)
        turned = jnp.transpose(keys[2 * i : 2 * i + 2, :, 4 * hd :].reshape(block, hv).astype(f32))
        valt[:, i * block : (i + 1) * block] = turned.astype(bf16)
        begin = i * (i + 1) // 2
        tiles = mix[begin : begin + i + 1].reshape((i + 1) * block, block)
        return jnp.dot(valt[:, : (i + 1) * block], tiles, preferred_element_type=f32)

    def settle(i, raw):
        size = lax.rsqrt(jnp.mean(raw * raw, axis=0, keepdims=True) + 1e-06)
        done = (jnp.transpose(raw * size) * hgain[...]).astype(bf16)
        hsend[2 * i : 2 * i + 2] = done.reshape(2, rows, hv)
        for dst in (2 * i, 2 * i + 1):

            @pl.when(dst != sp)
            def _():
                heads(dst, sp).start()

            @pl.when(dst == sp)
            def _():
                heads_in[:, pl.ds(pl.multiple_of(sp * hv, hv), hv)] = hsend[dst]

    def settle_all(which):
        raw = weigh(which[0])
        for n_th, i in enumerate(which):
            following = weigh(which[n_th + 1]) if n_th + 1 < len(which) else None
            settle(i, raw)
            raw = following

    done_to = 0
    top = score(0)
    for i in range(blocks):
        next_top = score(i + 1) if i + 1 < blocks else None
        normalize(i, top)
        top = next_top
        ready = {blocks - 3: i - 1, blocks - 2: i, blocks - 1: i + 1}.get(i, 0)
        if ready > done_to:
            settle_all(range(done_to, ready))
            done_to = ready

    mixed[...] = res[...].astype(f32)
    wo_a.wait()
    wo_b.wait()

    def project(g, carry):
        pair = (g // RING) * RING + (g % RING + 2 * (1 - g // RING)) % RING
        for s in range(2):
            src = 2 * pair + s

            @pl.when(src != sp)
            def _():
                heads(src, src).wait_recv()

        deep = pl.ds(pl.multiple_of(pair * 2 * hv, 2 * hv), 2 * hv)
        part = heads_in[:, deep]
        mixed[:, :half] += jnp.dot(part, wg[deep, :], preferred_element_type=f32)
        mixed[:, half:] += jnp.dot(part, wu[deep, :], preferred_element_type=f32)
        return carry

    lax.fori_loop(0, nsp // 2, project, 0)
    wg_c.start()
    wu_c.start()
    square = jnp.zeros((rows, 128), f32)
    for t in range(width // 128):
        value = mixed[:, t * 128 : (t + 1) * 128]
        square = square + value * value
    factor = lax.rsqrt(jnp.sum(square, axis=1, keepdims=True) / width + 1e-06)

    def gx(chunk, i, src):
        k = chunk[0]
        return remote(
            gath.at[dp, :, cols(chunk)], gath.at[src * 2 + c, :, cols(chunk)], xs.at[k, i], xr.at[k, i],
            (sp, xpeer(i) * 2 + c),
        )

    def gown(chunk, src):
        k = chunk[0]
        return remote(
            gath.at[dp, :, cols(chunk)], gath.at[src, :, cols(chunk)], cs.at[k, 3], cr.at[k, 3],
            (sp, partner),
        )

    def gfwd(chunk, i, core):
        k = chunk[0]
        at = xpeer(i, -1) * 2 + core
        return remote(
            gath.at[at, :, cols(chunk)], gath.at[at, :, cols(chunk)], cs.at[k, i], cr.at[k, i],
            (sp, partner),
        )

    def gsend(chunk):
        for i in (1, 0, 2):
            gx(chunk, i, x).start()
        gown(chunk, dp).start()

    widths = [EDGE] * ENDS + [WIDE] * wide + [EDGE] * ENDS
    static = [(k, sum(widths[:k]), w) for k, w in enumerate(widths)]
    for k, chunk in enumerate(static):
        at = slice(chunk[1], chunk[1] + chunk[2])
        gath[dp, :, at] = (mixed[:, at] * factor * gain[:, at]).astype(bf16)
        if k > 0:
            gsend(static[k - 1])
    gsend(static[-1])
    acc[...] = jnp.zeros_like(acc)

    def exchange(out_buf, in_buf, ssem, rsem, chunk, i, src, dst):
        k = chunk[0]
        return remote(
            out_buf.at[dst, :, cols(chunk)], in_buf.at[src, :, cols(chunk)],
            ssem.at[k, i], rsem.at[k, i], (dst, dp),
        )

    def send_all(out_buf, in_buf, ssem, rsem, chunk):
        for i in range(nsp - 1):
            exchange(out_buf, in_buf, ssem, rsem, chunk, i, sp, peer(i)).start()

    def wait_all(out_buf, in_buf, ssem, rsem, chunk):
        for i in range(nsp - 1):
            exchange(out_buf, in_buf, ssem, rsem, chunk, i, peer(i, -1), peer(i)).wait_recv()

    def dispatch(chunk):
        for i in (0, 2, 1):
            gx(chunk, i, xpeer(i, -1)).wait_recv()
            gfwd(chunk, i, c).start()
        gown(chunk, partner).wait_recv()
        for i in (0, 2, 1):
            gfwd(chunk, i, 1 - c).wait_recv()
        tokens = gath[:, :, cols(chunk)].reshape(ndp * rows, chunk[2])
        group = nsp // 4

        def build(g, carry):
            sel = pick[pl.ds(pl.multiple_of(g * group * slots, group * slots), group * slots), :]
            made = jnp.dot(sel, tokens, preferred_element_type=f32).astype(bf16)
            slab[pl.ds(g * group, group), :, cols(chunk)] = made.reshape(group, slots, chunk[2])
            return carry

        lax.fori_loop(0, 4, build, 0)
        xin[sp, :, cols(chunk)] = slab[sp, :, cols(chunk)]
        send_all(slab, xin, ds, dr, chunk)

    def each(action, end=n):
        loop(0, ENDS, lambda k: action(head_chunk(k)))
        loop(ENDS, ENDS + wide, lambda k: action(middle(k)))
        loop(ENDS + wide, end, lambda k: action(tail_chunk(k)))

    each(dispatch)
    wg_c.wait()
    wu_c.wait()
    tile = 256
    span = acc.shape[1]
    per = span // tile

    def receive(chunk):
        wait_all(slab, xin, ds, dr, chunk)

        def units(t, carry):
            at = pl.ds(pl.multiple_of(t * tile, tile), tile)
            to = pl.ds(pl.multiple_of((t % per) * tile, tile), tile)
            low = pl.ds(pl.multiple_of((t // per) * filled, filled), filled)
            high = pl.ds(pl.multiple_of((t // per + half // span) * filled, filled), filled)
            taken = xin[:, :, cols(chunk)].reshape(filled, chunk[2])
            gate = jnp.dot(taken, wg[cols(chunk), at], preferred_element_type=f32)
            upper = jnp.dot(taken, wu[cols(chunk), at], preferred_element_type=f32)
            acc[low, to] += gate
            acc[high, to] += upper
            return carry

        lax.fori_loop(0, half // tile, units, 0)

    each(receive, n - 1)

    wait_all(slab, xin, ds, dr, static[-1])

    def gated(t, carry):
        at = pl.ds(pl.multiple_of(t * tile, tile), tile)
        to = pl.ds(pl.multiple_of((t % per) * tile, tile), tile)
        low = pl.ds(pl.multiple_of((t // per) * filled, filled), filled)
        high = pl.ds(pl.multiple_of((t // per + half // span) * filled, filled), filled)
        taken = xin[:, :, cols(static[-1])].reshape(filled, EDGE)
        deep = cols(static[-1])
        gate = acc[low, to] + jnp.dot(taken, wg[deep, at], preferred_element_type=f32)
        upper = acc[high, to] + jnp.dot(taken, wu[deep, at], preferred_element_type=f32)
        gate = jnp.minimum(gate, 7.0)
        upper = jnp.clip(upper, -7.0, 7.0) + 1.0
        hid[:, at] = (upper * gate / (1.0 + jnp.exp(-1.702 * gate))).astype(bf16)
        return carry

    lax.fori_loop(0, half // tile, gated, 0)
    wd_c.wait()

    def down(chunk):
        made = jnp.dot(hid[...], wd[:, cols(chunk)], preferred_element_type=f32).astype(bf16)
        back[:, :, cols(chunk)] = made.reshape(nsp, slots, chunk[2])
        rin[sp, :, cols(chunk)] = back[sp, :, cols(chunk)]
        send_all(back, rin, bs, br, chunk)

    each(down)

    def part_copy(chunk):
        k = chunk[0]
        return remote(
            part_out.at[:, :, cols(chunk)], part_in.at[:, :, cols(chunk)], ps.at[k], pr.at[k],
            (sp, partner),
        )

    def total_copy(chunk, i, src):
        k = chunk[0]
        return remote(
            sum_out.at[xpeer(i), :, cols(chunk)], sum_in.at[src, :, cols(chunk)],
            ts.at[k, i], tr.at[k, i], (sp, xpeer(i) * 2 + c),
        )

    def weighted(core, chunk):
        sel = wsel[pl.ds(core * RING, RING)].reshape(RING * rows, filled)
        taken = rin[:, :, cols(chunk)].reshape(filled, chunk[2])
        made = jnp.dot(sel, taken, preferred_element_type=f32)
        return made.reshape(RING, rows, chunk[2])

    def out_copy(chunk):
        return pltpu.make_async_copy(
            done_out.at[:, cols(chunk)], out_hbm.at[:, cols(chunk)], osem.at[chunk[0]]
        )

    def combine(chunk):
        wait_all(back, rin, bs, br, chunk)
        part_out[:, :, cols(chunk)] = weighted(1 - c, chunk).astype(bf16)
        part_copy(chunk).start()
        own[chunk[0] % 2, :, :, : chunk[2]] = weighted(c, chunk)

    def add_parts(chunk):
        part_copy(chunk).wait_recv()
        mine = own.at[chunk[0] % 2]
        for i in (1, 0, 2):
            to = xpeer(i)
            sums = mine[to, :, : chunk[2]] + part_in[to, :, cols(chunk)].astype(f32)
            sum_out[to, :, cols(chunk)] = sums.astype(bf16)
        mixed[:, cols(chunk)] += mine[x, :, : chunk[2]] + part_in[x, :, cols(chunk)].astype(f32)
        for i in (1, 0, 2):
            total_copy(chunk, i, x).start()

    def finish(chunk):
        value = mixed[:, cols(chunk)]
        for i in range(3):
            total_copy(chunk, i, xpeer(i, -1)).wait_recv()
            value = value + sum_in[xpeer(i, -1), :, cols(chunk)].astype(f32)
        done_out[:, cols(chunk)] = value.astype(bf16)
        out_copy(chunk).start()

    def step(chunk, earlier=None):
        combine(chunk)
        if earlier is not None:
            finish(earlier)
        add_parts(chunk)

    begin, end = ENDS, ENDS + wide
    loop(0, begin, lambda k: step(head_chunk(k)))
    loop(begin, 2 * begin, lambda k: step(middle(k), head_chunk(k - ENDS)))
    loop(2 * begin, end, lambda k: step(middle(k), middle(k - ENDS)))
    loop(end, n, lambda k: step(tail_chunk(k)))
    loop(end - ENDS, end, lambda k: finish(middle(k)))

    for i in range(nsp - 1):
        qkv(peer(i), sp, 1).wait_send()
        heads(peer(i), sp).wait_send()
    for i in range(1, ndp):
        meta_copy(i, dp).wait_send()

    def left(chunk):
        for i in range(3):
            gx(chunk, i, x).wait_send()
            gfwd(chunk, i, c).wait_send()
        gown(chunk, dp).wait_send()
        part_copy(chunk).wait_send()
        for i in range(nsp - 1):
            exchange(slab, xin, ds, dr, chunk, i, sp, peer(i)).wait_send()
            exchange(back, rin, bs, br, chunk, i, sp, peer(i)).wait_send()

    def left_last(chunk):
        for i in range(3):
            total_copy(chunk, i, x).wait_send()
        out_copy(chunk).wait()

    each(left)
    each(left_last, end)
    loop(end, n, lambda k: finish(tail_chunk(k)))
    loop(end, n, lambda k: left_last(tail_chunk(k)))


def on_device(
    query_first,
    key_first,
    query_second,
    key_second,
    value_rows,
    mix_lambda,
    head_gain,
    residual,
    out_weight,
    norm_gain,
    routes,
    route_weights,
    gate_weight,
    up_weight,
    down_weight,
):
    nsp, ndp = lax.axis_size("sp"), lax.axis_size("dp")
    rows, width = residual.shape[1:]
    hidden = gate_weight.shape[2]
    qk = query_first.shape[2]
    hv = head_gain.shape[0]
    packed = 4 * qk // nsp + hv
    slots = CAP * ndp
    filled = slots * nsp
    n = (width - 2 * ENDS * EDGE) // WIDE + 2 * ENDS
    bf16, f32 = jnp.bfloat16, jnp.float32
    hbm = pl.BlockSpec(memory_space=pl.ANY)
    vmem = pltpu.VMEM
    dma = pltpu.SemaphoreType.DMA
    out = pl.pallas_call(
        layer_kernel,
        out_shape=jax.ShapeDtypeStruct((rows, width), bf16),
        in_specs=[hbm] * 15,
        out_specs=hbm,
        scratch_shapes=[
            vmem((rows, qk), bf16), vmem((rows, qk), bf16),
            vmem((rows, qk), bf16), vmem((rows, qk), bf16),
            vmem((rows, nsp * hv), bf16),
            vmem((1, nsp), f32), vmem((1, hv), f32), vmem((rows, width), bf16),
            vmem((1, width), f32), vmem((RING, rows), jnp.int32), vmem((RING, rows), f32),
            vmem((nsp, rows, packed), bf16),
            vmem((nsp, rows, packed), bf16),
            vmem((hv, nsp * rows), bf16),
            vmem((nsp * (nsp + 2) // 8, 2 * rows, 2 * rows), bf16),
            vmem((nsp, rows, hv), bf16),
            vmem((rows, nsp * hv), bf16),
            vmem((width, hidden), bf16), vmem((width, hidden), bf16),
            vmem((hidden, width), bf16),
            vmem((rows, width), f32),
            vmem((ndp, rows, width), bf16),
            vmem((nsp, slots, width), bf16), vmem((nsp, slots, width), bf16),
            vmem((max(4 * filled, (nsp - 1) * 2 * rows), hidden // 2), f32), vmem((filled, hidden), bf16),
            vmem((nsp, slots, width), bf16), vmem((nsp, slots, width), bf16),
            vmem((RING, rows, width), bf16), vmem((RING, rows, width), bf16),
            vmem((RING, rows, width), bf16), vmem((RING, rows, width), bf16),
            vmem((2, RING, rows, WIDE), f32),
            vmem((filled, ndp * rows), bf16),
            vmem((ndp, rows, filled), bf16),
            vmem((ndp, 8, rows), f32),
            vmem((rows, width), bf16),
            dma((11,)), dma((2, nsp)), dma((2, nsp)), dma((nsp,)), dma((nsp,)), dma((n,)),
            dma((5,)), dma((ndp,)), dma((ndp,)),
            dma((n, 3)), dma((n, 3)), dma((n, 4)), dma((n, 4)),
            dma((n, nsp)), dma((n, nsp)), dma((n, nsp)), dma((n, nsp)),
            dma((n,)), dma((n,)), dma((n, 3)), dma((n, 3)),
        ],
        compiler_params=pltpu.CompilerParams(
            collective_id=1, has_side_effects=True, vmem_limit_bytes=67000000
        ),
        name="layer",
    )(
        query_first[0], key_first[0], query_second[0], key_second[0], value_rows[0],
        mix_lambda[None, :], head_gain[None, :], residual[0], out_weight, norm_gain[None, :],
        routes[0].T, route_weights[0].T, gate_weight[0], up_weight[0], down_weight[0],
    )
    return out[None]


def solution(mesh):
    return jax.shard_map(
        on_device,
        mesh=mesh,
        in_specs=(
            P("dp", "sp", None),
            P("dp", "sp", None),
            P("dp", "sp", None),
            P("dp", "sp", None),
            P("dp", "sp", None),
            P(),
            P(),
            P("dp", "sp", None),
            P(),
            P(),
            P("dp", "sp", None),
            P("dp", "sp", None),
            P(("sp", "dp"), None, None),
            P(("sp", "dp"), None, None),
            P(("sp", "dp"), None, None),
        ),
        out_specs=P("dp", "sp", None),
        check_vma=False,
    )
```
